32 devices in a mesh: grp: 2 (over y), kv: 4 (over z), tp: 4 (over x, core).
Axes of the slice: x: 2, y: 2, z: 4, core: 2. Of those that a mesh axis runs over, the one named last changes fastest.
Arguments:
- tokens: bfloat16 [256, 4, 2048], P(('grp', 'kv'), None, 'tp'), parts along dimension 0, may hold values from -6 to 6
- in_gain: float32 [2048], replicated, may hold values from 0.1 to 1.9
- w_query: bfloat16 [2048, 1024], P('kv', 'tp'), may hold values from -0.125 to 0.125
- w_key: bfloat16 [2048, 1024], P('kv', 'tp'), may hold values from -0.125 to 0.125
- w_value: bfloat16 [2048, 1024], P('kv', 'tp'), may hold values from -0.125 to 0.125
- w_gate: bfloat16 [2048, 1024], P('kv', 'tp'), may hold values from -0.125 to 0.125
- w_beta: bfloat16 [2048, 16], replicated, may hold values from -0.125 to 0.125
- w_decay: bfloat16 [2048, 16], replicated, may hold values from -0.125 to 0.125
- decay_base: float32 [16], P('tp'), may hold values from 0.05 to 1
- out_gain: float32 [64], replicated, may hold values from 0.1 to 1.9
- w_out: bfloat16 [1024, 2048], P('tp', 'kv'), may hold values from -0.1875 to 0.1875
- state: float32 [256, 64, 1024], P(('grp', 'kv'), None, 'tp'), parts along dimension 0, may hold values from -0.8 to 0.8
- prev_keys: bfloat16 [256, 4, 1024], P(('grp', 'kv'), None, 'tp'), parts along dimension 0, may hold values from -6 to 6
- prev_values: bfloat16 [256, 4, 1024], P(('grp', 'kv'), None, 'tp'), parts along dimension 0, may hold values from -6 to 6
- prev_beta: float32 [256, 4, 16], P(('grp', 'kv'), None, 'tp'), parts along dimension 0, may hold values from -6 to 6
- prev_decay: float32 [256, 4, 16], P(('grp', 'kv'), None, 'tp'), parts along dimension 0, may hold values from -1 to -0.02
- accepted: int32 [256], P(('grp', 'kv')), parts along dimension 0, may hold values from 0 to 4
Outputs:
- mixed: bfloat16 [256, 4, 2048], P(('grp', 'kv'), None, 'tp'), parts along dimension 0
- new_state: float32 [256, 64, 1024], P(('grp', 'kv'), None, 'tp'), parts along dimension 0
The draws below stay inside these ranges and needn't reach their ends.
There are 2 independent parts, one for each index of `grp`. The reference program is written for one: setup_inputs(seed, part) draws one part's arguments, and reference() takes and returns one part's arrays. A program takes and returns all parts, laid end to end along the dimension named above; an argument that names none is the same for every part. Nothing has to cross between parts.
All inputs are finite; a program needn't handle non-finite values.
Results may differ from the reference program's by a relative error of at most 0.012.
Values may be sent and summed in bfloat16 or wider, within the bound.
A program may use at most 128 MiB of HBM per device.

```python
import math
import jax
import jax.numpy as jnp
from jax import lax

D = 2048
HEADS = 16
HD = 64
P_SIZE = 4
SEQ_DEV = 32
SEQS = 128
N_KV = 4


def plant(entries, rng, least, top_value):
    spot = [jax.random.randint(jax.random.fold_in(rng, axis), (), 0, length) for axis, length in enumerate(entries.shape)]
    widest = entries.shape.index(max(entries.shape))
    neighbour = spot[:widest] + [(spot[widest] + 1) % entries.shape[widest]] + spot[widest + 1:]
    return entries.at[tuple(spot)].set(least).at[tuple(neighbour)].set(top_value)


def shard_levels(stream_key, shape, cuts, smallest, high):
    gain = 1.0
    for axis_at, shards_of in cuts:
        draws = jax.random.uniform(jax.random.fold_in(jax.random.fold_in(stream_key, 6), axis_at), (shards_of,), jnp.float32, smallest / len(cuts), high / len(cuts))
        gain = gain * jnp.repeat(jnp.exp(draws), shape[axis_at] // shards_of).reshape((-1,) + (1,) * (len(shape) - 1 - axis_at))
    return gain


def centred(own_key, dims, scale, limit, split=(), kind=jnp.bfloat16):
    entries = scale * jax.random.normal(own_key, dims, jnp.float32)
    if split:
        entries = entries * shard_levels(own_key, dims, split, -0.22, 0.18)
    return jnp.clip(entries, -limit, limit).astype(kind)


def setup_inputs(seed: int = 0, part: int = 0) -> dict:
    splits = jax.random.split(jax.random.key(seed), 18)
    part_keys = jax.random.split(jax.random.fold_in(splits[17], part), 18)
    return {
        "tokens": centred(part_keys[0], (SEQS, P_SIZE, D), 1.0, 6.0, ((0, 4), (2, 4))),
        "in_gain": jnp.clip(1.0 + 0.18 * jax.random.normal(splits[1], (D,), jnp.float32), 0.1, 1.9),
        "w_query": centred(splits[2], (D, HEADS * HD), D ** -0.5, 0.125, ((0, 4), (1, 4))),
        "w_key": centred(splits[3], (D, HEADS * HD), D ** -0.5, 0.125, ((0, 4), (1, 4))),
        "w_value": centred(splits[4], (D, HEADS * HD), D ** -0.5, 0.125, ((0, 4), (1, 4))),
        "w_gate": centred(splits[5], (D, HEADS * HD), D ** -0.5, 0.125, ((0, 4), (1, 4))),
        "w_beta": centred(splits[6], (D, HEADS), D ** -0.5, 0.125),
        "w_decay": centred(splits[7], (D, HEADS), D ** -0.5, 0.125),
        "decay_base": jnp.clip(jnp.exp(math.log(1.0) - 2.9957323 * jax.random.uniform(splits[8], (HEADS,), jnp.float32) ** shard_levels(splits[8], (HEADS,), ((0, 4),), -0.2, 0.2)), 0.05, 1.0),
        "out_gain": jnp.clip(1.0 + 0.18 * jax.random.normal(splits[9], (HD,), jnp.float32), 0.1, 1.9),
        "w_out": centred(splits[10], (HEADS * HD, D), (HEADS * HD) ** -0.5, 0.1875, ((0, 4), (1, 4))),
        "state": centred(part_keys[11], (SEQS, HD, HEADS * HD), 0.1, 0.8, ((0, 4), (2, 4)), jnp.float32),
        "prev_keys": centred(part_keys[12], (SEQS, P_SIZE, HEADS * HD), 1.0, 6.0, ((0, 4), (2, 4))),
        "prev_values": centred(part_keys[13], (SEQS, P_SIZE, HEADS * HD), 1.0, 6.0, ((0, 4), (2, 4))),
        "prev_beta": centred(part_keys[14], (SEQS, P_SIZE, HEADS), 1.5, 6.0, ((0, 4), (2, 4)), jnp.float32),
        "prev_decay": jnp.clip(-1.0 + 0.98 * jax.random.uniform(part_keys[15], (SEQS, P_SIZE, HEADS), jnp.float32) ** shard_levels(part_keys[15], (SEQS, P_SIZE, HEADS), ((0, 4), (2, 4)), -0.2, 0.2), -1.0, -0.02),
        "accepted": plant(jax.random.randint(part_keys[16], (SEQS,), 0, P_SIZE + 1), jax.random.fold_in(part_keys[16], 1), 0, P_SIZE).astype(jnp.int32),
    }


EPS = 1e-06

def normalize_rows(vector):
    return vector * lax.rsqrt(lax.optimization_barrier(jnp.sum(vector * vector, -1, keepdims=True)) + EPS)

def delta_block(saved, queries, keys_in, values_in, strength, log_decay):
    highest = lax.Precision.HIGHEST
    steps_len = queries.shape[1]
    cumul = jnp.transpose(jnp.cumsum(log_decay, axis=1), (0, 2, 1))
    q_heads = jnp.transpose(queries, (0, 2, 1, 3))
    k_heads = jnp.transpose(keys_in, (0, 2, 1, 3))
    v_heads = jnp.transpose(values_in, (0, 2, 1, 3))
    weight_t = jnp.transpose(strength, (0, 2, 1))
    spread = cumul[..., :, None] - cumul[..., None, :]
    order = jnp.arange(steps_len)
    inside = order[:, None] >= order[None, :]
    below = order[:, None] > order[None, :]
    dec_incl = jnp.where(inside, jnp.exp(jnp.where(inside, spread, 0.0)), 0.0)
    dec_strict = jnp.where(below, dec_incl, 0.0)
    lower_mat = weight_t[..., :, None] * jnp.einsum('bhik,bhjk->bhij', k_heads, k_heads, precision=highest) * dec_strict
    growth = jnp.exp(cumul)
    rhs_all = jnp.concatenate([weight_t[..., None] * v_heads, (weight_t * growth)[..., None] * k_heads], axis=-1)
    solved = []
    for row_index in range(steps_len):
        current = rhs_all[:, :, row_index]
        for col_index in range(row_index):
            current = current - lower_mat[:, :, row_index, col_index, None] * solved[col_index]
        solved.append(current)
    solution = jnp.stack(solved, axis=2)
    value_size = v_heads.shape[-1]
    update = solution[..., :value_size] - jnp.einsum('bhpk,bhkv->bhpv', solution[..., value_size:], saved, precision=highest)
    scores = jnp.einsum('bhik,bhjk->bhij', q_heads, k_heads, precision=highest) * dec_incl
    output = jnp.einsum('bhpk,bhkv->bhpv', growth[..., None] * q_heads, saved, precision=highest) + jnp.einsum('bhij,bhjv->bhiv', scores, update, precision=highest)
    tail = jnp.exp(cumul[..., -1:] - cumul)[..., None] * k_heads
    renewed = jnp.exp(cumul[..., -1])[..., None, None] * saved + jnp.einsum('bhpk,bhpv->bhkv', tail, update, precision=highest)
    return (jnp.transpose(output, (0, 2, 1, 3)), renewed)

def reference(tokens, in_gain, w_query, w_key, w_value, w_gate, w_beta, w_decay, decay_base, out_gain, w_out, state, prev_keys, prev_values, prev_beta, prev_decay, accepted):
    rows = SEQS * P_SIZE
    wide = tokens.astype(jnp.float32)
    normed = (wide * lax.rsqrt(lax.optimization_barrier(jnp.mean(wide * wide, -1, keepdims=True)) + EPS) * in_gain).astype(jnp.bfloat16)
    flat = normed.reshape(rows, D)
    shape4 = (SEQS, P_SIZE, HEADS, HD)
    query = normalize_rows(jnp.dot(flat, w_query, preferred_element_type=jnp.float32).reshape(shape4)) * HD ** (-0.5)
    key_vec = normalize_rows(jnp.dot(flat, w_key, preferred_element_type=jnp.float32).reshape(shape4))
    value_vec = jnp.dot(flat, w_value, preferred_element_type=jnp.float32).reshape(shape4)
    gate = jnp.dot(flat, w_gate, preferred_element_type=jnp.float32).reshape(shape4)
    strength = jax.nn.sigmoid(jnp.dot(flat, w_beta, preferred_element_type=jnp.float32)).reshape(SEQS, P_SIZE, HEADS)
    log_decay = (-decay_base * jax.nn.softplus(jnp.dot(flat, w_decay, preferred_element_type=jnp.float32))).reshape(SEQS, P_SIZE, HEADS)
    live = (jnp.arange(P_SIZE, dtype=jnp.int32)[None, :] < accepted[:, None]).astype(jnp.float32)
    prev_strength = jax.nn.sigmoid(prev_beta) * live[..., None]
    prev_log = prev_decay * live[..., None]
    prev_k = normalize_rows(prev_keys.astype(jnp.float32).reshape(shape4))
    prev_v = prev_values.astype(jnp.float32).reshape(shape4)
    saved = jnp.transpose(state.reshape(SEQS, HD, HEADS, HD), (0, 2, 1, 3))

    def per_block(inputs):
        held, pk_in, pv_in, pb_in, pg_in, qu_in, ke_in, va_in, st_in, lg_in = inputs
        committed = delta_block(held, pk_in, pk_in, pv_in, pb_in, pg_in)[1]
        output = delta_block(committed, qu_in, ke_in, va_in, st_in, lg_in)[0]
        return (output, committed)
    pieces = (saved, prev_k, prev_v, prev_strength, prev_log, query, key_vec, value_vec, strength, log_decay)
    blocked = tuple((array.reshape((N_KV, SEQ_DEV) + array.shape[1:]) for array in pieces))
    output, committed = lax.map(per_block, blocked)
    output = output.reshape(shape4)
    committed = committed.reshape(SEQS, HEADS, HD, HD)
    gated = (output * lax.rsqrt(lax.optimization_barrier(jnp.mean(output * output, -1, keepdims=True)) + EPS) * out_gain * jax.nn.silu(gate)).astype(jnp.bfloat16).reshape(rows, HEADS * HD)
    mixed = jnp.dot(gated, w_out, preferred_element_type=jnp.float32).astype(jnp.bfloat16).reshape(SEQS, P_SIZE, D)
    new_state = jnp.transpose(committed, (0, 2, 1, 3)).reshape(SEQS, HD, HEADS * HD)
    return (mixed, new_state)
```

```python
import functools

import jax
import jax.numpy as jnp
from jax import lax
from jax.experimental import pallas as pl
from jax.experimental.pallas import tpu as pltpu
from jax.sharding import PartitionSpec as P

EPS = 1e-06
F32 = jnp.float32
BF16 = jnp.bfloat16
MESH = pl.DeviceIdType.MESH


def kernel(
    cfg,
    tok_hbm, gain_ref, wq_hbm, wk_hbm, wv_hbm, wg_hbm, wb_ref, wd_ref, base_ref, og_ref, wo_hbm,
    state_hbm, pk_ref, pv_ref, pb_ref, pd_ref, acc_ref,
    mixed_ref, new_hbm,
    tok, wp, wo, st, normed, kq, res, tk, up, al, rows_a, rows_b, proj, send_buf, recv_buf,
    in_sem, own_sem, zr_send, zl_send, z_recv, y_send, y_recv, t_send, t_recv, r_send, r_recv,
    out_sem,
):
    n_grp, n_kv, n_tp, seqs, props, heads, hd, gather_out = cfg
    width = heads * hd
    g = lax.axis_index("grp")
    k = lax.axis_index("kv")
    t_me = lax.axis_index("tp")
    rows = seqs * props
    own_rows = wk_hbm.shape[0]
    piece = own_rows // n_grp
    out_piece = wo.shape[1] // n_grp
    sources = [wk_hbm, wq_hbm, wv_hbm, wg_hbm]
    n_mat = len(sources) + (1 if gather_out else 0)

    tok_in = pltpu.make_async_copy(tok_hbm, tok.at[t_me], in_sem.at[0])
    tok_in.start()
    own_copies = []
    for m in range(n_mat):
        if m < len(sources):
            dst = wp.at[m, pl.ds(k * own_rows, own_rows), :]
            copy = pltpu.make_async_copy(sources[m], dst, own_sem.at[m])
        else:
            copy = pltpu.make_async_copy(wo_hbm, wo.at[k], own_sem.at[m])
        copy.start()
        own_copies.append(copy)
    state_in = pltpu.make_async_copy(state_hbm, st, in_sem.at[1])
    state_in.start()
    out_in = None
    if not gather_out:
        out_in = pltpu.make_async_copy(wo_hbm, wo, own_sem.at[n_mat])
        out_in.start()

    barrier = pltpu.get_barrier_semaphore()

    def greet(dev):
        pl.semaphore_signal(barrier, inc=1, device_id=dev, device_id_type=MESH)

    @pl.when(k > 0)
    def _():
        greet({"kv": k - 1})

    @pl.when(k < n_kv - 1)
    def _():
        greet({"kv": k + 1})

    for d in range(1, n_grp):
        greet({"grp": lax.rem(g + d, n_grp)})
    for d in range(1, n_tp):
        greet({"tp": lax.rem(t_me + d, n_tp)})

    beside = jnp.minimum(k, 1) + jnp.minimum(n_kv - 1 - k, 1)
    pl.semaphore_wait(barrier, n_grp + n_tp - 2 + beside)

    def slot(m, origin, part):
        if m < len(sources):
            return wp.at[m, pl.ds(origin * own_rows + part * piece, piece), :]
        return wo.at[origin, pl.ds(part * out_piece, out_piece), :]

    def z_right(m, origin):
        ref = slot(m, origin, g)
        return pltpu.make_async_remote_copy(
            ref, ref, zr_send.at[m, origin], z_recv.at[m, origin],
            device_id={"kv": k + 1}, device_id_type=MESH)

    def z_left(m, origin):
        ref = slot(m, origin, g)
        return pltpu.make_async_remote_copy(
            ref, ref, zl_send.at[m, origin], z_recv.at[m, origin],
            device_id={"kv": k - 1}, device_id_type=MESH)

    def y_copy(m, origin, d):
        ref = slot(m, origin, g)
        return pltpu.make_async_remote_copy(
            ref, ref, y_send.at[d - 1, m, origin], y_recv.at[d - 1, m, origin],
            device_id={"grp": lax.rem(g + d, n_grp)}, device_id_type=MESH)

    def y_wait(m, origin, d):
        ref = slot(m, origin, lax.rem(g + n_grp - d, n_grp))
        pltpu.make_async_remote_copy(
            ref, ref, y_send.at[d - 1, m, origin], y_recv.at[d - 1, m, origin],
            device_id={"grp": lax.rem(g + d, n_grp)}, device_id_type=MESH).wait_recv()

    def send_own(m):
        own_copies[m].wait()

        @pl.when(k < n_kv - 1)
        def _():
            z_right(m, k).start()

        @pl.when(k > 0)
        def _():
            z_left(m, k).start()

    def forward(m):
        def step(s, carry):
            left = k - 1 - s
            right = k + 1 + s

            @pl.when(left >= 0)
            def _():
                z_right(m, left).wait_recv()

                @pl.when(k < n_kv - 1)
                def _():
                    z_right(m, left).start()

                for d in range(1, n_grp):
                    y_copy(m, left, d).start()

            @pl.when(right < n_kv)
            def _():
                z_left(m, right).wait_recv()

                @pl.when(k > 0)
                def _():
                    z_left(m, right).start()

                for d in range(1, n_grp):
                    y_copy(m, right, d).start()

            return carry

        lax.fori_loop(0, n_kv - 1, step, 0)

    def wait_y(m):
        def step(o, carry):
            @pl.when(o != k)
            def _():
                for d in range(1, n_grp):
                    y_wait(m, o, d)

            return carry

        lax.fori_loop(0, n_kv, step, 0)

    def t_copy(d):
        return pltpu.make_async_remote_copy(
            tok.at[t_me], tok.at[t_me], t_send.at[d - 1], t_recv.at[d - 1],
            device_id={"tp": lax.rem(t_me + d, n_tp)}, device_id_type=MESH)

    def t_wait(d):
        origin = lax.rem(t_me + n_tp - d, n_tp)
        pltpu.make_async_remote_copy(
            tok.at[origin], tok.at[origin], t_send.at[d - 1], t_recv.at[d - 1],
            device_id={"tp": lax.rem(t_me + d, n_tp)}, device_id_type=MESH).wait_recv()

    send_own(0)
    tok_in.wait()
    for d in range(1, n_tp):
        t_copy(d).start()
    send_own(1)

    blk = (
        lax.broadcasted_iota(jnp.int32, (width, width), 0) // hd
        == lax.broadcasted_iota(jnp.int32, (width, width), 1) // hd
    ).astype(F32).astype(BF16)
    lane_head = lax.broadcasted_iota(jnp.int32, (1, width), 1) // hd
    masks = [(lane_head == h).astype(F32) for h in range(heads)]

    def head_sum(x):
        hi = x.astype(BF16)
        lo = (x - hi.astype(F32)).astype(BF16)
        return jnp.dot(hi, blk, preferred_element_type=F32) + jnp.dot(
            lo, blk, preferred_element_type=F32)

    lanes = 128
    blocks = width // lanes

    def rd(ref, at, *lead):
        return jnp.concatenate([ref[(*lead, c, at)] for c in range(blocks)], axis=-1)

    def wr(ref, at, x, *lead):
        for c in range(blocks):
            ref[(*lead, c, at)] = x[:, c * lanes : (c + 1) * lanes]

    every = pl.ds(0, rows)

    def spread(x):
        total = jnp.zeros((x.shape[0], width), F32)
        for h in range(heads):
            total = jnp.where(lane_head == h, x[:, h : h + 1], total)
        return total

    pad = 2 * props

    def by_state(s, carry):
        tile = st[pl.ds(pl.multiple_of(s * hd, hd), hd), :]
        stacked = jnp.concatenate([(tile * mask).astype(BF16) for mask in masks], axis=0)
        at = pl.ds(pl.multiple_of(s * pad, pad), pad)
        lhs = rd(kq, at).astype(BF16)
        wr(res, at, jnp.dot(lhs, stacked, preferred_element_type=F32))
        return carry

    def solve(keys, values, weights, logs, queries):
        cumul = []
        run = None
        for t in range(props):
            run = logs[t] if run is None else run + logs[t]
            cumul.append(run)
        low = [(i, j) for i in range(props) for j in range(i)]
        products = [keys[i] * keys[j] for i, j in low]
        full = []
        if queries is not None:
            full = [(i, j) for i in range(props) for j in range(i + 1)]
            products += [queries[i] * keys[j] for i, j in full]
        sums = head_sum(jnp.concatenate(products, axis=0))
        sums = [sums[i * seqs : (i + 1) * seqs] for i in range(len(products))]
        kk = dict(zip(low, sums))
        qk = dict(zip(full, sums[len(low):]))
        dec = {pair: jnp.exp(cumul[pair[0]] - cumul[pair[1]]) for pair in low}
        growth = [jnp.exp(c) for c in cumul]
        update = []
        for t in range(props):
            seen = rd(res, pl.ds(t, seqs, stride=pad))
            term = values[t] - growth[t] * seen
            for j in range(t):
                term = term - kk[t, j] * dec[t, j] * update[j]
            update.append(weights[t] * term)
        outs = []
        if queries is not None:
            for t in range(props):
                out = growth[t] * rd(res, pl.ds(props + t, seqs, stride=pad))
                for j in range(t + 1):
                    score = qk[t, j] if j == t else qk[t, j] * dec[t, j]
                    out = out + score * update[j]
                outs.append(out)
        return cumul, growth, update, outs

    def split(ref):
        return [rd(ref, pl.ds(t, seqs, stride=props)) for t in range(props)]

    pk = pk_ref[...].astype(F32)
    wr(rows_a, every, pk * lax.rsqrt(head_sum(pk * pk) + EPS))
    wr(rows_b, every, pv_ref[...].astype(F32))
    keys = split(rows_a)
    values = split(rows_b)
    accepted = jnp.broadcast_to(acc_ref[...], (seqs, width))
    weights, logs = [], []
    for t in range(props):
        live = (accepted > t).astype(F32)
        weights.append(spread(jax.nn.sigmoid(pb_ref[:, t, :])) * live)
        logs.append(spread(pd_ref[:, t, :]) * live)
        wr(kq, pl.ds(t, seqs, stride=pad), keys[t])
        wr(kq, pl.ds(props + t, seqs, stride=pad), keys[t])
    state_in.wait()
    lax.fori_loop(0, seqs, by_state, 0, unroll=4)
    cumul, growth, update, _ = solve(keys, values, weights, logs, None)
    al[...] = growth[-1]
    for t in range(props):
        wr(tk, pl.ds(t, seqs, stride=pad), jnp.exp(cumul[-1] - cumul[t]) * keys[t])
        wr(up, pl.ds(t, seqs, stride=pad), update[t])
        wr(tk, pl.ds(props + t, seqs, stride=pad), jnp.zeros((seqs, width), F32))
        wr(up, pl.ds(props + t, seqs, stride=pad), jnp.zeros((seqs, width), F32))

    def renew(s, carry):
        at = pl.ds(pl.multiple_of(s * pad, pad), pad)
        outer = lax.dot_general(
            rd(tk, at), rd(up, at), (((0,), (0,)), ((), ())), preferred_element_type=F32)
        where = pl.ds(pl.multiple_of(s * hd, hd), hd)
        tile = al[pl.ds(s, 1), :] * st[where, :]
        for h in range(heads):
            tile = tile + masks[h] * outer[h * hd : (h + 1) * hd, :]
        st[where, :] = tile
        return carry

    lax.fori_loop(0, seqs, renew, 0, unroll=2)
    state_out = pltpu.make_async_copy(st, new_hbm, out_sem)
    state_out.start()

    for d in range(1, n_tp):
        t_wait(d)
    square = jnp.zeros((rows, 1), F32)
    for i in range(n_tp):
        wide = tok[i].astype(F32)
        square = square + jnp.sum(wide * wide, -1, keepdims=True)
    feats = tok.shape[2]
    scale = lax.rsqrt(square / (n_tp * feats) + EPS)
    for i in range(n_tp):
        cols = slice(i * feats, (i + 1) * feats)
        normed[:, cols] = (tok[i].astype(F32) * scale * gain_ref[:, cols]).astype(BF16)
    all_heads = wb_ref.shape[1]
    pick = (
        lax.broadcasted_iota(jnp.int32, (all_heads, width), 0)
        == t_me * heads + lax.broadcasted_iota(jnp.int32, (all_heads, width), 1) // hd
    ).astype(F32)

    def per_head(ref):
        raw = jnp.dot(normed[...], ref[...], preferred_element_type=F32)
        return jnp.dot(raw, pick, precision=lax.Precision.HIGHEST, preferred_element_type=F32)

    wr(rows_a, every, jax.nn.sigmoid(per_head(wb_ref)))
    weights = split(rows_a)
    base = jnp.zeros((1, width), F32)
    for h in range(heads):
        base = jnp.where(lane_head == h, base_ref[h], base)
    wr(rows_b, every, -base * jax.nn.softplus(per_head(wd_ref)))
    logs = split(rows_b)

    def project(m):
        return jnp.dot(normed[...], wp[m], preferred_element_type=F32)

    def finish(m):
        wait_y(m)
        if m < len(sources):
            value = project(m)
            if m == 0:
                value = value * lax.rsqrt(head_sum(value * value) + EPS)
            elif m == 1:
                value = value * lax.rsqrt(head_sum(value * value) + EPS) * hd ** (-0.5)
            wr(proj, every, value, m)

    outs = None
    for m in range(n_mat):
        if m >= 1 and m + 1 < n_mat:
            send_own(m + 1)
        forward(m)
        if m >= 1:
            finish(m - 1)
        if m == 3:
            keys = [rd(proj, pl.ds(t, seqs, stride=props), 0) for t in range(props)]
            queries = [rd(proj, pl.ds(t, seqs, stride=props), 1) for t in range(props)]
            values = [rd(proj, pl.ds(t, seqs, stride=props), 2) for t in range(props)]
            for t in range(props):
                wr(kq, pl.ds(t, seqs, stride=pad), keys[t])
                wr(kq, pl.ds(props + t, seqs, stride=pad), queries[t])
            lax.fori_loop(0, seqs, by_state, 0, unroll=4)
            outs = solve(keys, values, weights, logs, queries)[3]
            for t in range(props):
                wr(rows_a, pl.ds(t, seqs, stride=props), outs[t])
            out = rd(rows_a, every)
            out = out * lax.rsqrt(head_sum(out * out) / hd + EPS)
            tile_gain = (
                lax.broadcasted_iota(jnp.int32, (hd, width), 0)
                == lax.broadcasted_iota(jnp.int32, (hd, width), 1) % hd
            ).astype(F32)
            gain = jnp.dot(
                jnp.broadcast_to(og_ref[...], (8, hd)), tile_gain,
                precision=lax.Precision.HIGHEST, preferred_element_type=F32)[:1]
            wr(rows_a, every, out * gain)
    if not gather_out:
        finish(n_mat - 1)
        out_in.wait()
    gate = rd(proj, every, 3)
    gated = (rd(rows_a, every) * (gate / (1.0 + jnp.exp(-gate)))).astype(BF16)
    if gather_out:
        finish(n_mat - 1)

    def r_copy(d):
        dest = lax.rem(t_me + d, n_tp)
        return pltpu.make_async_remote_copy(
            send_buf.at[d - 1], recv_buf.at[d - 1], r_send.at[d - 1], r_recv.at[d - 1],
            device_id={"tp": dest}, device_id_type=MESH)

    order = sorted(range(1, n_tp), key=lambda d: -min(d, n_tp - d))
    for d in order:
        dest = lax.rem(t_me + d, n_tp)
        send_buf[d - 1] = jnp.dot(gated, wo[dest], preferred_element_type=F32).astype(BF16)
        r_copy(d).start()
    total = jnp.dot(gated, wo[t_me], preferred_element_type=F32)
    for d in reversed(order):
        r_copy(d).wait_recv()
        total = total + recv_buf[d - 1].astype(F32)
    mixed_ref[...] = total.astype(BF16)

    for d in range(1, n_tp):
        t_copy(d).wait_send()
        r_copy(d).wait_send()

    def drain(m):
        def step(o, carry):
            @pl.when(jnp.logical_and(o <= k, k < n_kv - 1))
            def _():
                z_right(m, o).wait_send()

            @pl.when(jnp.logical_and(o >= k, k > 0))
            def _():
                z_left(m, o).wait_send()

            @pl.when(o != k)
            def _():
                for d in range(1, n_grp):
                    y_copy(m, o, d).wait_send()

            return carry

        lax.fori_loop(0, n_kv, step, 0)

    for m in range(n_mat):
        drain(m)
    state_out.wait()


def body(
    sizes,
    tokens, in_gain, w_query, w_key, w_value, w_gate, w_beta, w_decay, decay_base, out_gain, w_out,
    state, prev_keys, prev_values, prev_beta, prev_decay, accepted,
):
    n_grp, n_kv, n_tp = sizes
    seqs, props, feats = tokens.shape
    heads = decay_base.shape[0]
    hd = out_gain.shape[0]
    width = heads * hd
    rows = seqs * props
    pad = 2 * props
    gather_out = n_kv == n_tp
    if not gather_out:
        w_out = lax.all_gather(w_out, "kv", axis=1, tiled=True)
        w_out = jnp.transpose(w_out.reshape(width, n_tp, feats), (1, 0, 2))
    n_mat = 5 if gather_out else 4
    cfg = (n_grp, n_kv, n_tp, seqs, props, heads, hd, gather_out)
    vmem = pl.BlockSpec(memory_space=pltpu.VMEM)
    hbm = pl.BlockSpec(memory_space=pl.ANY)
    smem = pl.BlockSpec(memory_space=pltpu.SMEM)
    dma = pltpu.SemaphoreType.DMA
    mixed, new_state = pl.pallas_call(
        functools.partial(kernel, cfg),
        out_shape=(
            jax.ShapeDtypeStruct((rows, feats), BF16),
            jax.ShapeDtypeStruct((seqs * hd, width), F32),
        ),
        in_specs=[hbm, vmem, hbm, hbm, hbm, hbm, vmem, vmem, smem, vmem, hbm, hbm,
                  vmem, vmem, vmem, vmem, vmem],
        out_specs=(vmem, hbm),
        scratch_shapes=[
            pltpu.VMEM((n_tp, rows, feats), BF16),
            pltpu.VMEM((4, n_kv * w_key.shape[0], width), BF16),
            pltpu.VMEM((n_tp, width, feats), BF16),
            pltpu.VMEM((seqs * hd, width), F32),
            pltpu.VMEM((rows, n_tp * feats), BF16),
            pltpu.VMEM((width // 128, seqs * pad, 128), F32),
            pltpu.VMEM((width // 128, seqs * pad, 128), F32),
            pltpu.VMEM((width // 128, seqs * pad, 128), F32),
            pltpu.VMEM((width // 128, seqs * pad, 128), F32),
            pltpu.VMEM((seqs, width), F32),
            pltpu.VMEM((width // 128, rows, 128), F32),
            pltpu.VMEM((width // 128, rows, 128), F32),
            pltpu.VMEM((4, width // 128, rows, 128), F32),
            pltpu.VMEM((n_tp - 1, rows, feats), BF16),
            pltpu.VMEM((n_tp - 1, rows, feats), BF16),
            dma((2,)),
            dma((6,)),
            dma((n_mat, n_kv)),
            dma((n_mat, n_kv)),
            dma((n_mat, n_kv)),
            dma((max(n_grp - 1, 1), n_mat, n_kv)),
            dma((max(n_grp - 1, 1), n_mat, n_kv)),
            dma((n_tp - 1,)),
            dma((n_tp - 1,)),
            dma((n_tp - 1,)),
            dma((n_tp - 1,)),
            dma(()),
        ],
        compiler_params=pltpu.CompilerParams(
            collective_id=0, has_side_effects=True, vmem_limit_bytes=48 * 2**20),
    )(
        tokens.reshape(rows, feats), in_gain.reshape(1, -1), w_query, w_key, w_value, w_gate,
        w_beta, w_decay, decay_base, out_gain.reshape(1, -1), w_out,
        state.reshape(seqs * hd, width), prev_keys.reshape(rows, width),
        prev_values.reshape(rows, width), prev_beta, prev_decay, accepted.reshape(seqs, 1),
    )
    return mixed.reshape(seqs, props, feats), new_state.reshape(seqs, hd, width)


def solution(mesh):
    sizes = (mesh.shape["grp"], mesh.shape["kv"], mesh.shape["tp"])
    tokens = P(("grp", "kv"), None, "tp")
    placed = (
        tokens, P(), P("kv", "tp"), P("kv", "tp"), P("kv", "tp"), P("kv", "tp"), P(), P(),
        P("tp"), P(), P("tp", "kv"), tokens, tokens, tokens, tokens, tokens, P(("grp", "kv")),
    )
    return jax.shard_map(
        functools.partial(body, sizes),
        mesh=mesh,
        in_specs=placed,
        out_specs=(tokens, tokens),
        check_vma=False,
    )
```

```python
import functools

import jax
import jax.numpy as jnp
from jax import lax
from jax.experimental import pallas as pl
from jax.experimental.pallas import tpu as pltpu
from jax.sharding import PartitionSpec as P

EPS = 1e-06
F32 = jnp.float32
BF16 = jnp.bfloat16
MESH = pl.DeviceIdType.MESH


def kernel(
    cfg,
    tok_hbm, gain_hbm, wq_hbm, wk_hbm, wv_hbm, wg_hbm, wb_hbm, wd_hbm, base_hbm, og_hbm, wo_hbm,
    state_hbm, pk_hbm, pv_hbm, pb_hbm, pd_hbm, acc_hbm,
    mixed_ref, new_hbm,
    gain_ref, wb_ref, wd_ref, base_ref, og_ref, pk_ref, pv_ref, pb_ref, pd_ref, acc_ref, tok, wp, wo, st, normed, kq, res, tk, up, al, rows_a, rows_b, proj, send_buf, recv_buf, gate_buf, own_share,
    in_sem, own_sem, zr_send, zl_send, z_recv, y_send, y_recv, t_send, t_recv, r_send, r_recv,
    out_sem, small_sem,
):
    n_grp, n_kv, n_tp, seqs, props, heads, hd, gather_out = cfg
    width = heads * hd
    g = lax.axis_index("grp")
    k = lax.axis_index("kv")
    t_me = lax.axis_index("tp")
    rows = seqs * props
    own_rows = wk_hbm.shape[0]
    piece = own_rows // n_grp
    out_piece = wo.shape[1] // n_grp
    sources = [wk_hbm, wq_hbm, wv_hbm, wg_hbm]
    n_mat = len(sources) + (1 if gather_out else 0)

    tok_in = pltpu.make_async_copy(tok_hbm, tok.at[t_me], in_sem.at[0])
    tok_in.start()
    own_copies = []
    for m in range(n_mat):
        if m < len(sources):
            dst = wp.at[m, pl.ds(k * own_rows, own_rows), :]
            copy = pltpu.make_async_copy(sources[m], dst, own_sem.at[m])
        else:
            copy = pltpu.make_async_copy(wo_hbm, wo.at[k], own_sem.at[m])
        copy.start()
        own_copies.append(copy)
    early, late = [], []
    pairs = [
        (pk_hbm, pk_ref, early), (pv_hbm, pv_ref, early), (pb_hbm, pb_ref, early),
        (pd_hbm, pd_ref, early), (acc_hbm, acc_ref, early), (gain_hbm, gain_ref, late),
        (wb_hbm, wb_ref, late), (wd_hbm, wd_ref, late), (base_hbm, base_ref, late),
        (og_hbm, og_ref, late),
    ]
    for i, (src, dst, group) in enumerate(pairs):
        copy = pltpu.make_async_copy(src, dst, small_sem.at[i])
        copy.start()
        group.append(copy)
    state_in = pltpu.make_async_copy(state_hbm, st, in_sem.at[1])
    state_in.start()
    out_in = None
    if not gather_out:
        out_in = pltpu.make_async_copy(wo_hbm, wo, own_sem.at[n_mat])
        out_in.start()

    barrier = pltpu.get_barrier_semaphore()

    def greet(dev):
        pl.semaphore_signal(barrier, inc=1, device_id=dev, device_id_type=MESH)

    @pl.when(k > 0)
    def _():
        greet({"kv": k - 1})

    @pl.when(k < n_kv - 1)
    def _():
        greet({"kv": k + 1})

    for d in range(1, n_grp):
        greet({"grp": lax.rem(g + d, n_grp)})
    for d in range(1, n_tp):
        greet({"tp": lax.rem(t_me + d, n_tp)})

    beside = jnp.minimum(k, 1) + jnp.minimum(n_kv - 1 - k, 1)
    pl.semaphore_wait(barrier, n_grp + n_tp - 2 + beside)

    def slot(m, origin, part):
        if m < len(sources):
            return wp.at[m, pl.ds(origin * own_rows + part * piece, piece), :]
        return wo.at[origin, pl.ds(part * out_piece, out_piece), :]

    def z_right(m, origin):
        ref = slot(m, origin, g)
        return pltpu.make_async_remote_copy(
            ref, ref, zr_send.at[m, origin], z_recv.at[m, origin],
            device_id={"kv": k + 1}, device_id_type=MESH)

    def z_left(m, origin):
        ref = slot(m, origin, g)
        return pltpu.make_async_remote_copy(
            ref, ref, zl_send.at[m, origin], z_recv.at[m, origin],
            device_id={"kv": k - 1}, device_id_type=MESH)

    def y_copy(m, origin, d):
        ref = slot(m, origin, g)
        return pltpu.make_async_remote_copy(
            ref, ref, y_send.at[d - 1, m, origin], y_recv.at[d - 1, m, origin],
            device_id={"grp": lax.rem(g + d, n_grp)}, device_id_type=MESH)

    def y_wait(m, origin, d):
        ref = slot(m, origin, lax.rem(g + n_grp - d, n_grp))
        pltpu.make_async_remote_copy(
            ref, ref, y_send.at[d - 1, m, origin], y_recv.at[d - 1, m, origin],
            device_id={"grp": lax.rem(g + d, n_grp)}, device_id_type=MESH).wait_recv()

    def send_own(m):
        own_copies[m].wait()

        @pl.when(k < n_kv - 1)
        def _():
            z_right(m, k).start()

        @pl.when(k > 0)
        def _():
            z_left(m, k).start()

    def forward_step(m, s):
        left = k - 1 - s
        right = k + 1 + s

        @pl.when(left >= 0)
        def _():
            z_right(m, left).wait_recv()

            @pl.when(k < n_kv - 1)
            def _():
                z_right(m, left).start()

            for d in range(1, n_grp):
                y_copy(m, left, d).start()

        @pl.when(right < n_kv)
        def _():
            z_left(m, right).wait_recv()

            @pl.when(k > 0)
            def _():
                z_left(m, right).start()

            for d in range(1, n_grp):
                y_copy(m, right, d).start()

    def forward(m):
        def step(s, carry):
            forward_step(m, s)
            return carry

        lax.fori_loop(0, n_kv - 1, step, 0)

    def wait_y(m):
        def step(o, carry):
            @pl.when(o != k)
            def _():
                for d in range(1, n_grp):
                    y_wait(m, o, d)

            return carry

        lax.fori_loop(0, n_kv, step, 0)

    def t_copy(d):
        return pltpu.make_async_remote_copy(
            tok.at[t_me], tok.at[t_me], t_send.at[d - 1], t_recv.at[d - 1],
            device_id={"tp": lax.rem(t_me + d, n_tp)}, device_id_type=MESH)

    def t_wait(d):
        origin = lax.rem(t_me + n_tp - d, n_tp)
        pltpu.make_async_remote_copy(
            tok.at[origin], tok.at[origin], t_send.at[d - 1], t_recv.at[d - 1],
            device_id={"tp": lax.rem(t_me + d, n_tp)}, device_id_type=MESH).wait_recv()

    send_own(0)
    tok_in.wait()
    for d in range(1, n_tp):
        t_copy(d).start()
    send_own(1)

    blk = (
        lax.broadcasted_iota(jnp.int32, (width, width), 0) // hd
        == lax.broadcasted_iota(jnp.int32, (width, width), 1) // hd
    ).astype(F32).astype(BF16)
    lane_head = lax.broadcasted_iota(jnp.int32, (1, width), 1) // hd
    masks = [(lane_head == h).astype(F32) for h in range(heads)]

    def head_sum(x):
        hi = x.astype(BF16)
        lo = (x - hi.astype(F32)).astype(BF16)
        return jnp.dot(hi, blk, preferred_element_type=F32) + jnp.dot(
            lo, blk, preferred_element_type=F32)

    lanes = 128
    blocks = width // lanes

    def rd(ref, at, *lead):
        return jnp.concatenate([ref[(*lead, c, at)] for c in range(blocks)], axis=-1)

    def wr(ref, at, x, *lead):
        for c in range(blocks):
            ref[(*lead, c, at)] = x[:, c * lanes : (c + 1) * lanes]

    every = pl.ds(0, rows)

    pad = 2 * props

    def by_state(s, carry):
        tile = st[pl.ds(pl.multiple_of(s * hd, hd), hd), :]
        stacked = jnp.concatenate([(tile * mask).astype(BF16) for mask in masks], axis=0)
        at = pl.ds(pl.multiple_of(s * pad, pad), pad)
        lhs = rd(kq, at).astype(BF16)
        wr(res, at, jnp.dot(lhs, stacked, preferred_element_type=F32))
        return carry

    def solve(keys, values, weights, logs, queries):
        cumul = []
        run = None
        for t in range(props):
            run = logs[t] if run is None else run + logs[t]
            cumul.append(run)
        low = [(i, j) for i in range(props) for j in range(i)]
        products = [keys[i] * keys[j] for i, j in low]
        full = []
        if queries is not None:
            full = [(i, j) for i in range(props) for j in range(i + 1)]
            products += [queries[i] * keys[j] for i, j in full]
        sums = head_sum(jnp.concatenate(products, axis=0))
        sums = [sums[i * seqs : (i + 1) * seqs] for i in range(len(products))]
        kk = dict(zip(low, sums))
        qk = dict(zip(full, sums[len(low):]))
        dec = {pair: jnp.exp(cumul[pair[0]] - cumul[pair[1]]) for pair in low}
        growth = [jnp.exp(c) for c in cumul]
        update = []
        for t in range(props):
            seen = rd(res, pl.ds(t, seqs, stride=pad))
            term = values[t] - growth[t] * seen
            for j in range(t):
                term = term - kk[t, j] * dec[t, j] * update[j]
            update.append(weights[t] * term)
        outs = []
        if queries is not None:
            for t in range(props):
                out = growth[t] * rd(res, pl.ds(props + t, seqs, stride=pad))
                for j in range(t + 1):
                    score = qk[t, j] if j == t else qk[t, j] * dec[t, j]
                    out = out + score * update[j]
                outs.append(out)
        return cumul, growth, update, outs

    def split(ref):
        return [rd(ref, pl.ds(t, seqs, stride=props)) for t in range(props)]

    for copy in early:
        copy.wait()
    pk = pk_ref[...].astype(F32).reshape(rows, width)
    wr(rows_a, every, pk * lax.rsqrt(head_sum(pk * pk) + EPS))
    wr(rows_b, every, pv_ref[...].astype(F32).reshape(rows, width))
    keys = split(rows_a)
    values = split(rows_b)
    own_head = (
        lax.broadcasted_iota(jnp.int32, (heads, width), 0)
        == lax.broadcasted_iota(jnp.int32, (heads, width), 1) // hd
    ).astype(F32)

    def over_lanes(x):
        return lax.dot_general(
            x, own_head, (((0,), (0,)), ((), ())),
            precision=lax.Precision.HIGHEST, preferred_element_type=F32)

    weights, logs = [], []
    for t in range(props):
        live = (acc_ref[...] > t).astype(F32)
        weights.append(over_lanes(jax.nn.sigmoid(pb_ref[t]) * live))
        logs.append(over_lanes(pd_ref[t] * live))
        wr(kq, pl.ds(t, seqs, stride=pad), keys[t])
        wr(kq, pl.ds(props + t, seqs, stride=pad), keys[t])
    state_in.wait()
    lax.fori_loop(0, seqs, by_state, 0, unroll=4)
    cumul, growth, update, _ = solve(keys, values, weights, logs, None)
    al[...] = growth[-1]
    for t in range(props):
        wr(tk, pl.ds(t, seqs, stride=pad), jnp.exp(cumul[-1] - cumul[t]) * keys[t])
        wr(up, pl.ds(t, seqs, stride=pad), update[t])
        wr(tk, pl.ds(props + t, seqs, stride=pad), jnp.zeros((seqs, width), F32))
        wr(up, pl.ds(props + t, seqs, stride=pad), jnp.zeros((seqs, width), F32))

    def renew(s, carry):
        at = pl.ds(pl.multiple_of(s * pad, pad), pad)
        outer = lax.dot_general(
            rd(tk, at), rd(up, at), (((0,), (0,)), ((), ())), preferred_element_type=F32)
        where = pl.ds(pl.multiple_of(s * hd, hd), hd)
        tile = al[pl.ds(s, 1), :] * st[where, :]
        for h in range(heads):
            tile = tile + masks[h] * outer[h * hd : (h + 1) * hd, :]
        st[where, :] = tile
        return carry

    lax.fori_loop(0, seqs, renew, 0, unroll=2)
    state_out = pltpu.make_async_copy(st, new_hbm, out_sem)
    state_out.start()

    for d in range(1, n_tp):
        t_wait(d)
    for copy in late:
        copy.wait()
    square = jnp.zeros((rows, 1), F32)
    for i in range(n_tp):
        wide = tok[i].astype(F32).reshape(rows, -1)
        square = square + jnp.sum(wide * wide, -1, keepdims=True)
    feats = tok.shape[3]
    scale = lax.rsqrt(square / (n_tp * feats) + EPS)
    for i in range(n_tp):
        cols = slice(i * feats, (i + 1) * feats)
        normed[:, cols] = (tok[i].astype(F32).reshape(rows, -1) * scale * gain_ref[:, cols]).astype(BF16)
    all_heads = wb_ref.shape[0]
    pick = (
        lax.broadcasted_iota(jnp.int32, (all_heads, width), 0)
        == t_me * heads + lax.broadcasted_iota(jnp.int32, (all_heads, width), 1) // hd
    ).astype(F32)

    def per_head(ref):
        raw = lax.dot_general(
            normed[...], ref[...], (((1,), (1,)), ((), ())), preferred_element_type=F32)
        return jnp.dot(raw, pick, precision=lax.Precision.HIGHEST, preferred_element_type=F32)

    wr(rows_a, every, jax.nn.sigmoid(per_head(wb_ref)))
    weights = split(rows_a)
    base = jnp.zeros((1, width), F32)
    for h in range(heads):
        base = jnp.where(lane_head == h, base_ref[:, h : h + 1], base)
    wr(rows_b, every, -base * jax.nn.softplus(per_head(wd_ref)))
    logs = split(rows_b)

    def project(m):
        return jnp.dot(normed[...], wp[m], preferred_element_type=F32)

    def finish(m):
        wait_y(m)
        if m < len(sources):
            value = project(m)
            if m == 0:
                value = value * lax.rsqrt(head_sum(value * value) + EPS)
            elif m == 1:
                value = value * lax.rsqrt(head_sum(value * value) + EPS) * hd ** (-0.5)
            wr(proj, every, value, m)

    outs = None
    def r_copy(dest):
        return pltpu.make_async_remote_copy(
            send_buf.at[dest], recv_buf.at[t_me], r_send.at[dest], r_recv.at[t_me],
            device_id={"tp": dest}, device_id_type=MESH)

    def r_wait(origin):
        pltpu.make_async_remote_copy(
            send_buf.at[origin], recv_buf.at[origin], r_send.at[origin], r_recv.at[origin],
            device_id={"tp": origin}, device_id_type=MESH).wait_recv()

    def send_share(dest):
        share = jnp.dot(gate_buf[...], wo[dest], preferred_element_type=F32)

        @pl.when(dest == t_me)
        def _():
            own_share[...] = share

        @pl.when(dest != t_me)
        def _():
            send_buf[dest] = share.astype(BF16)
            r_copy(dest).start()

    for m in range(len(sources)):
        if m >= 1 and m + 1 < n_mat:
            send_own(m + 1)
        forward(m)
        if m >= 1:
            finish(m - 1)
        if m == 3:
            keys = [rd(proj, pl.ds(t, seqs, stride=props), 0) for t in range(props)]
            queries = [rd(proj, pl.ds(t, seqs, stride=props), 1) for t in range(props)]
            values = [rd(proj, pl.ds(t, seqs, stride=props), 2) for t in range(props)]
            for t in range(props):
                wr(kq, pl.ds(t, seqs, stride=pad), keys[t])
                wr(kq, pl.ds(props + t, seqs, stride=pad), queries[t])
            lax.fori_loop(0, seqs, by_state, 0, unroll=4)
            outs = solve(keys, values, weights, logs, queries)[3]
            for t in range(props):
                wr(rows_a, pl.ds(t, seqs, stride=props), outs[t])
            out = rd(rows_a, every)
            out = out * lax.rsqrt(head_sum(out * out) / hd + EPS)
            tile_gain = (
                lax.broadcasted_iota(jnp.int32, (hd, width), 0)
                == lax.broadcasted_iota(jnp.int32, (hd, width), 1) % hd
            ).astype(F32)
            gain = jnp.dot(
                jnp.broadcast_to(og_ref[...], (8, hd)), tile_gain,
                precision=lax.Precision.HIGHEST, preferred_element_type=F32)[:1]
            wr(rows_a, every, out * gain)
    finish(len(sources) - 1)
    gate = rd(proj, every, 3)
    gate_buf[...] = (rd(rows_a, every) * (gate / (1.0 + jnp.exp(-gate)))).astype(BF16)
    if gather_out:
        m = n_mat - 1

        def take(s, carry):
            @pl.when(s < n_kv - 1)
            def _():
                forward_step(m, s)

            @pl.when(k - s >= 0)
            def _():
                @pl.when(s > 0)
                def _():
                    for d in range(1, n_grp):
                        y_wait(m, k - s, d)

                send_share(k - s)

            @pl.when(jnp.logical_and(s > 0, k + s < n_kv))
            def _():
                for d in range(1, n_grp):
                    y_wait(m, k + s, d)
                send_share(k + s)

            return carry

        lax.fori_loop(0, n_kv, take, 0)
    else:
        out_in.wait()
        for d in range(n_tp):
            send_share(lax.rem(t_me + d, n_tp))
    total = own_share[...]
    for d in range(1, n_tp):
        origin = lax.rem(t_me + d, n_tp)
        r_wait(origin)
        total = total + recv_buf[origin].astype(F32)
    mixed_ref[...] = total.reshape(seqs, props, feats).astype(BF16)

    for d in range(1, n_tp):
        t_copy(d).wait_send()
        r_copy(lax.rem(t_me + d, n_tp)).wait_send()

    def drain(m):
        def step(o, carry):
            @pl.when(jnp.logical_and(o <= k, k < n_kv - 1))
            def _():
                z_right(m, o).wait_send()

            @pl.when(jnp.logical_and(o >= k, k > 0))
            def _():
                z_left(m, o).wait_send()

            @pl.when(o != k)
            def _():
                for d in range(1, n_grp):
                    y_copy(m, o, d).wait_send()

            return carry

        lax.fori_loop(0, n_kv, step, 0)

    for m in range(n_mat):
        drain(m)
    state_out.wait()


def body(
    sizes,
    tokens, in_gain, w_query, w_key, w_value, w_gate, w_beta, w_decay, decay_base, out_gain, w_out,
    state, prev_keys, prev_values, prev_beta, prev_decay, accepted,
):
    n_grp, n_kv, n_tp = sizes
    seqs, props, feats = tokens.shape
    heads = decay_base.shape[0]
    hd = out_gain.shape[0]
    width = heads * hd
    rows = seqs * props
    pad = 2 * props
    gather_out = n_kv == n_tp
    if not gather_out:
        w_out = lax.all_gather(w_out, "kv", axis=1, tiled=True)
        w_out = jnp.transpose(w_out.reshape(width, n_tp, feats), (1, 0, 2))
    n_mat = 5 if gather_out else 4
    cfg = (n_grp, n_kv, n_tp, seqs, props, heads, hd, gather_out)
    vmem = pl.BlockSpec(memory_space=pltpu.VMEM)
    hbm = pl.BlockSpec(memory_space=pl.ANY)
    args = (
        tokens, in_gain.reshape(1, -1), w_query, w_key, w_value, w_gate,
        w_beta.T, w_decay.T, decay_base.reshape(1, -1), out_gain.reshape(1, -1), w_out,
        state.reshape(seqs * hd, width), prev_keys, prev_values,
        jnp.transpose(prev_beta, (1, 2, 0)), jnp.transpose(prev_decay, (1, 2, 0)),
        accepted.reshape(1, seqs),
    )
    dma = pltpu.SemaphoreType.DMA
    mixed, new_state = pl.pallas_call(
        functools.partial(kernel, cfg),
        out_shape=(
            jax.ShapeDtypeStruct((seqs, props, feats), BF16),
            jax.ShapeDtypeStruct((seqs * hd, width), F32),
        ),
        in_specs=[hbm] * len(args),
        out_specs=(vmem, hbm),
        scratch_shapes=[
            *[pltpu.VMEM(args[i].shape, args[i].dtype) for i in (1, 6, 7, 8, 9, 12, 13, 14, 15, 16)],
            pltpu.VMEM((n_tp, seqs, props, feats), BF16),
            pltpu.VMEM((4, n_kv * w_key.shape[0], width), BF16),
            pltpu.VMEM((n_tp, width, feats), BF16),
            pltpu.VMEM((seqs * hd, width), F32),
            pltpu.VMEM((rows, n_tp * feats), BF16),
            pltpu.VMEM((width // 128, seqs * pad, 128), F32),
            pltpu.VMEM((width // 128, seqs * pad, 128), F32),
            pltpu.VMEM((width // 128, seqs * pad, 128), F32),
            pltpu.VMEM((width // 128, seqs * pad, 128), F32),
            pltpu.VMEM((seqs, width), F32),
            pltpu.VMEM((width // 128, rows, 128), F32),
            pltpu.VMEM((width // 128, rows, 128), F32),
            pltpu.VMEM((4, width // 128, rows, 128), F32),
            pltpu.VMEM((n_tp, rows, feats), BF16),
            pltpu.VMEM((n_tp, rows, feats), BF16),
            pltpu.VMEM((rows, width), BF16),
            pltpu.VMEM((rows, feats), F32),
            dma((2,)),
            dma((6,)),
            dma((n_mat, n_kv)),
            dma((n_mat, n_kv)),
            dma((n_mat, n_kv)),
            dma((max(n_grp - 1, 1), n_mat, n_kv)),
            dma((max(n_grp - 1, 1), n_mat, n_kv)),
            dma((n_tp - 1,)),
            dma((n_tp - 1,)),
            dma((n_tp,)),
            dma((n_tp,)),
            dma(()),
            dma((10,)),
        ],
        compiler_params=pltpu.CompilerParams(
            collective_id=0, has_side_effects=True, vmem_limit_bytes=67043328),
    )(*args)
    return mixed, new_state.reshape(seqs, hd, width)


def solution(mesh):
    sizes = (mesh.shape["grp"], mesh.shape["kv"], mesh.shape["tp"])
    tokens = P(("grp", "kv"), None, "tp")
    placed = (
        tokens, P(), P("kv", "tp"), P("kv", "tp"), P("kv", "tp"), P("kv", "tp"), P(), P(),
        P("tp"), P(), P("tp", "kv"), tokens, tokens, tokens, tokens, tokens, P(("grp", "kv")),
    )
    return jax.shard_map(
        functools.partial(body, sizes),
        mesh=mesh,
        in_specs=placed,
        out_specs=(tokens, tokens),
        check_vma=False,
    )
```

```python
import functools

import jax
import jax.numpy as jnp
from jax import lax
from jax.experimental import pallas as pl
from jax.experimental.pallas import tpu as pltpu
from jax.sharding import PartitionSpec as P

EPS = 1e-06
F32 = jnp.float32
BF16 = jnp.bfloat16
MESH = pl.DeviceIdType.MESH


def kernel(
    cfg,
    tok_hbm, gain_hbm, wq_hbm, wk_hbm, wv_hbm, wg_hbm, wb_hbm, wd_hbm, base_hbm, og_hbm, wo_hbm,
    state_hbm, pk_hbm, pv_hbm, pb_hbm, pd_hbm, acc_hbm,
    mixed_ref, st,
    gain_ref, wb_ref, wd_ref, base_ref, og_ref, pk_ref, pv_ref, pb_ref, pd_ref, acc_ref, tok, wp, wo, normed, kq, res, tk, up, al, rows_a, rows_b, proj, send_buf, recv_buf, gate_buf, own_share,
    in_sem, own_sem, zr_send, zl_send, z_recv, y_send, y_recv, t_send, t_recv, r_send, r_recv,
    small_sem,
):
    n_grp, n_kv, n_tp, seqs, props, heads, hd, gather_out = cfg
    width = heads * hd
    g = lax.axis_index("grp")
    k = lax.axis_index("kv")
    t_me = lax.axis_index("tp")
    rows = seqs * props
    own_rows = wk_hbm.shape[0]
    piece = own_rows // n_grp
    out_piece = wo.shape[1] // n_grp
    sources = [wk_hbm, wq_hbm, wv_hbm, wg_hbm]
    n_mat = len(sources) + (1 if gather_out else 0)

    tok_in = pltpu.make_async_copy(tok_hbm, tok.at[t_me], in_sem.at[0])
    tok_in.start()
    own_copies = []
    for m in range(n_mat):
        if m < len(sources):
            dst = wp.at[m, pl.ds(k * own_rows, own_rows), :]
            copy = pltpu.make_async_copy(sources[m], dst, own_sem.at[m])
        else:
            copy = pltpu.make_async_copy(wo_hbm, wo.at[k], own_sem.at[m])
        copy.start()
        own_copies.append(copy)
    early, late = [], []
    pairs = [
        (pk_hbm, pk_ref, early), (pv_hbm, pv_ref, early), (pb_hbm, pb_ref, early),
        (pd_hbm, pd_ref, early), (acc_hbm, acc_ref, early), (gain_hbm, gain_ref, late),
        (wb_hbm, wb_ref, late), (wd_hbm, wd_ref, late), (base_hbm, base_ref, late),
        (og_hbm, og_ref, late),
    ]
    for i, (src, dst, group) in enumerate(pairs):
        copy = pltpu.make_async_copy(src, dst, small_sem.at[i])
        copy.start()
        group.append(copy)
    state_in = pltpu.make_async_copy(state_hbm, st, in_sem.at[1])
    state_in.start()
    out_in = None
    if not gather_out:
        out_in = pltpu.make_async_copy(wo_hbm, wo, own_sem.at[n_mat])
        out_in.start()

    barrier = pltpu.get_barrier_semaphore()

    def greet(dev):
        pl.semaphore_signal(barrier, inc=1, device_id=dev, device_id_type=MESH)

    @pl.when(k > 0)
    def _():
        greet({"kv": k - 1})

    @pl.when(k < n_kv - 1)
    def _():
        greet({"kv": k + 1})

    for d in range(1, n_grp):
        greet({"grp": lax.rem(g + d, n_grp)})
    for d in range(1, n_tp):
        greet({"tp": lax.rem(t_me + d, n_tp)})

    beside = jnp.minimum(k, 1) + jnp.minimum(n_kv - 1 - k, 1)
    pl.semaphore_wait(barrier, n_grp + n_tp - 2 + beside)

    def slot(m, origin, part):
        if m < len(sources):
            return wp.at[m, pl.ds(origin * own_rows + part * piece, piece), :]
        return wo.at[origin, pl.ds(part * out_piece, out_piece), :]

    def z_right(m, origin):
        ref = slot(m, origin, g)
        return pltpu.make_async_remote_copy(
            ref, ref, zr_send.at[m, origin], z_recv.at[m, origin],
            device_id={"kv": k + 1}, device_id_type=MESH)

    def z_left(m, origin):
        ref = slot(m, origin, g)
        return pltpu.make_async_remote_copy(
            ref, ref, zl_send.at[m, origin], z_recv.at[m, origin],
            device_id={"kv": k - 1}, device_id_type=MESH)

    def y_copy(m, origin, d):
        ref = slot(m, origin, g)
        return pltpu.make_async_remote_copy(
            ref, ref, y_send.at[d - 1, m, origin], y_recv.at[d - 1, m, origin],
            device_id={"grp": lax.rem(g + d, n_grp)}, device_id_type=MESH)

    def y_wait(m, origin, d):
        ref = slot(m, origin, lax.rem(g + n_grp - d, n_grp))
        pltpu.make_async_remote_copy(
            ref, ref, y_send.at[d - 1, m, origin], y_recv.at[d - 1, m, origin],
            device_id={"grp": lax.rem(g + d, n_grp)}, device_id_type=MESH).wait_recv()

    def send_own(m):
        own_copies[m].wait()

        @pl.when(k < n_kv - 1)
        def _():
            z_right(m, k).start()

        @pl.when(k > 0)
        def _():
            z_left(m, k).start()

    def forward_step(m, s):
        left = k - 1 - s
        right = k + 1 + s

        @pl.when(left >= 0)
        def _():
            z_right(m, left).wait_recv()

            @pl.when(k < n_kv - 1)
            def _():
                z_right(m, left).start()

            for d in range(1, n_grp):
                y_copy(m, left, d).start()

        @pl.when(right < n_kv)
        def _():
            z_left(m, right).wait_recv()

            @pl.when(k > 0)
            def _():
                z_left(m, right).start()

            for d in range(1, n_grp):
                y_copy(m, right, d).start()

    def forward(m):
        def step(s, carry):
            forward_step(m, s)
            return carry

        lax.fori_loop(0, n_kv - 1, step, 0)

    def wait_y(m):
        def step(o, carry):
            @pl.when(o != k)
            def _():
                for d in range(1, n_grp):
                    y_wait(m, o, d)

            return carry

        lax.fori_loop(0, n_kv, step, 0)

    def t_copy(d):
        return pltpu.make_async_remote_copy(
            tok.at[t_me], tok.at[t_me], t_send.at[d - 1], t_recv.at[d - 1],
            device_id={"tp": lax.rem(t_me + d, n_tp)}, device_id_type=MESH)

    def t_wait(d):
        origin = lax.rem(t_me + n_tp - d, n_tp)
        pltpu.make_async_remote_copy(
            tok.at[origin], tok.at[origin], t_send.at[d - 1], t_recv.at[d - 1],
            device_id={"tp": lax.rem(t_me + d, n_tp)}, device_id_type=MESH).wait_recv()

    send_own(0)
    tok_in.wait()
    for d in range(1, n_tp):
        t_copy(d).start()
    send_own(1)
    send_own(2)

    blk = (
        lax.broadcasted_iota(jnp.int32, (width, width), 0) // hd
        == lax.broadcasted_iota(jnp.int32, (width, width), 1) // hd
    ).astype(F32).astype(BF16)
    lane_head = lax.broadcasted_iota(jnp.int32, (1, width), 1) // hd
    masks = [(lane_head == h).astype(F32) for h in range(heads)]

    def head_sum(x):
        hi = x.astype(BF16)
        lo = (x - hi.astype(F32)).astype(BF16)
        return jnp.dot(hi, blk, preferred_element_type=F32) + jnp.dot(
            lo, blk, preferred_element_type=F32)

    lanes = 128
    blocks = width // lanes

    def rd(ref, at, *lead):
        return jnp.concatenate([ref[(*lead, c, at)] for c in range(blocks)], axis=-1)

    def wr(ref, at, x, *lead):
        for c in range(blocks):
            ref[(*lead, c, at)] = x[:, c * lanes : (c + 1) * lanes]

    every = pl.ds(0, rows)

    pad = 2 * props

    def by_state(s, carry):
        tile = st[pl.ds(pl.multiple_of(s * hd, hd), hd), :]
        stacked = jnp.concatenate([(tile * mask).astype(BF16) for mask in masks], axis=0)
        at = pl.ds(pl.multiple_of(s * pad, pad), pad)
        lhs = rd(kq, at).astype(BF16)
        wr(res, at, jnp.dot(lhs, stacked, preferred_element_type=F32))
        return carry

    def solve(keys, values, weights, logs, queries):
        cumul = []
        run = None
        for t in range(props):
            run = logs[t] if run is None else run + logs[t]
            cumul.append(run)
        low = [(i, j) for i in range(props) for j in range(i)]
        products = [keys[i] * keys[j] for i, j in low]
        full = []
        if queries is not None:
            full = [(i, j) for i in range(props) for j in range(i + 1)]
            products += [queries[i] * keys[j] for i, j in full]
        sums = head_sum(jnp.concatenate(products, axis=0))
        sums = [sums[i * seqs : (i + 1) * seqs] for i in range(len(products))]
        kk = dict(zip(low, sums))
        qk = dict(zip(full, sums[len(low):]))
        dec = {pair: jnp.exp(cumul[pair[0]] - cumul[pair[1]]) for pair in low}
        growth = [jnp.exp(c) for c in cumul]
        update = []
        for t in range(props):
            seen = rd(res, pl.ds(t, seqs, stride=pad))
            term = values[t] - growth[t] * seen
            for j in range(t):
                term = term - kk[t, j] * dec[t, j] * update[j]
            update.append(weights[t] * term)
        outs = []
        if queries is not None:
            for t in range(props):
                out = growth[t] * rd(res, pl.ds(props + t, seqs, stride=pad))
                for j in range(t + 1):
                    score = qk[t, j] if j == t else qk[t, j] * dec[t, j]
                    out = out + score * update[j]
                outs.append(out)
        return cumul, growth, update, outs

    def split(ref):
        return [rd(ref, pl.ds(t, seqs, stride=props)) for t in range(props)]

    for copy in early:
        copy.wait()
    pk = pk_ref[...].astype(F32).reshape(rows, width)
    wr(rows_a, every, pk * lax.rsqrt(head_sum(pk * pk) + EPS))
    wr(rows_b, every, pv_ref[...].astype(F32).reshape(rows, width))
    keys = split(rows_a)
    values = split(rows_b)
    own_head = (
        lax.broadcasted_iota(jnp.int32, (heads, width), 0)
        == lax.broadcasted_iota(jnp.int32, (heads, width), 1) // hd
    ).astype(F32)

    def over_lanes(x):
        return lax.dot_general(
            x, own_head, (((0,), (0,)), ((), ())),
            precision=lax.Precision.HIGHEST, preferred_element_type=F32)

    weights, logs = [], []
    for t in range(props):
        live = (acc_ref[...] > t).astype(F32)
        weights.append(over_lanes(jax.nn.sigmoid(pb_ref[t]) * live))
        logs.append(over_lanes(pd_ref[t] * live))
        wr(kq, pl.ds(t, seqs, stride=pad), keys[t])
        wr(kq, pl.ds(props + t, seqs, stride=pad), keys[t])
    state_in.wait()
    lax.fori_loop(0, seqs, by_state, 0, unroll=4)
    cumul, growth, update, _ = solve(keys, values, weights, logs, None)
    al[...] = growth[-1]
    for t in range(props):
        wr(tk, pl.ds(t, seqs, stride=pad), jnp.exp(cumul[-1] - cumul[t]) * keys[t])
        wr(up, pl.ds(t, seqs, stride=pad), update[t])
        wr(tk, pl.ds(props + t, seqs, stride=pad), jnp.zeros((seqs, width), F32))
        wr(up, pl.ds(props + t, seqs, stride=pad), jnp.zeros((seqs, width), F32))

    def renew(s, carry):
        at = pl.ds(pl.multiple_of(s * pad, pad), pad)
        outer = lax.dot_general(
            rd(tk, at), rd(up, at), (((0,), (0,)), ((), ())), preferred_element_type=F32)
        where = pl.ds(pl.multiple_of(s * hd, hd), hd)
        tile = al[pl.ds(s, 1), :] * st[where, :]
        for h in range(heads):
            tile = tile + masks[h] * outer[h * hd : (h + 1) * hd, :]
        st[where, :] = tile
        return carry

    forward(0)
    send_own(3)
    lax.fori_loop(0, seqs // 2, renew, 0, unroll=2)
    forward(1)
    if gather_out:
        send_own(n_mat - 1)
    lax.fori_loop(seqs // 2, seqs, renew, 0, unroll=2)

    for d in range(1, n_tp):
        t_wait(d)
    for copy in late:
        copy.wait()
    square = jnp.zeros((rows, 1), F32)
    for i in range(n_tp):
        wide = tok[i].astype(F32).reshape(rows, -1)
        square = square + jnp.sum(wide * wide, -1, keepdims=True)
    feats = tok.shape[3]
    scale = lax.rsqrt(square / (n_tp * feats) + EPS)
    for i in range(n_tp):
        cols = slice(i * feats, (i + 1) * feats)
        normed[:, cols] = (tok[i].astype(F32).reshape(rows, -1) * scale * gain_ref[:, cols]).astype(BF16)
    all_heads = wb_ref.shape[0]
    pick = (
        lax.broadcasted_iota(jnp.int32, (all_heads, width), 0)
        == t_me * heads + lax.broadcasted_iota(jnp.int32, (all_heads, width), 1) // hd
    ).astype(F32)

    def per_head(ref):
        raw = lax.dot_general(
            normed[...], ref[...], (((1,), (1,)), ((), ())), preferred_element_type=F32)
        return jnp.dot(raw, pick, precision=lax.Precision.HIGHEST, preferred_element_type=F32)

    wr(rows_a, every, jax.nn.sigmoid(per_head(wb_ref)))
    weights = split(rows_a)
    base = jnp.zeros((1, width), F32)
    for h in range(heads):
        base = jnp.where(lane_head == h, base_ref[:, h : h + 1], base)
    wr(rows_b, every, -base * jax.nn.softplus(per_head(wd_ref)))
    logs = split(rows_b)

    def project(m):
        return jnp.dot(normed[...], wp[m], preferred_element_type=F32)

    def finish(m):
        wait_y(m)
        if m < len(sources):
            value = project(m)
            if m == 0:
                value = value * lax.rsqrt(head_sum(value * value) + EPS)
            elif m == 1:
                value = value * lax.rsqrt(head_sum(value * value) + EPS) * hd ** (-0.5)
            wr(proj, every, value, m)

    outs = None
    def r_copy(dest):
        return pltpu.make_async_remote_copy(
            send_buf.at[dest], recv_buf.at[t_me], r_send.at[dest], r_recv.at[t_me],
            device_id={"tp": dest}, device_id_type=MESH)

    def r_wait(origin):
        pltpu.make_async_remote_copy(
            send_buf.at[origin], recv_buf.at[origin], r_send.at[origin], r_recv.at[origin],
            device_id={"tp": origin}, device_id_type=MESH).wait_recv()

    def send_share(dest):
        share = jnp.dot(gate_buf[...], wo[dest], preferred_element_type=F32)

        @pl.when(dest == t_me)
        def _():
            own_share[...] = share

        @pl.when(dest != t_me)
        def _():
            send_buf[dest] = share.astype(BF16)
            r_copy(dest).start()

    for m in range(len(sources)):
        if m >= 2:
            forward(m)
        if m >= 1:
            finish(m - 1)
        if m == 3:
            keys = [rd(proj, pl.ds(t, seqs, stride=props), 0) for t in range(props)]
            queries = [rd(proj, pl.ds(t, seqs, stride=props), 1) for t in range(props)]
            values = [rd(proj, pl.ds(t, seqs, stride=props), 2) for t in range(props)]
            for t in range(props):
                wr(kq, pl.ds(t, seqs, stride=pad), keys[t])
                wr(kq, pl.ds(props + t, seqs, stride=pad), queries[t])
            lax.fori_loop(0, seqs, by_state, 0, unroll=4)
            outs = solve(keys, values, weights, logs, queries)[3]
            for t in range(props):
                wr(rows_a, pl.ds(t, seqs, stride=props), outs[t])
            out = rd(rows_a, every)
            out = out * lax.rsqrt(head_sum(out * out) / hd + EPS)
            tile_gain = (
                lax.broadcasted_iota(jnp.int32, (hd, width), 0)
                == lax.broadcasted_iota(jnp.int32, (hd, width), 1) % hd
            ).astype(F32)
            gain = jnp.dot(
                jnp.broadcast_to(og_ref[...], (8, hd)), tile_gain,
                precision=lax.Precision.HIGHEST, preferred_element_type=F32)[:1]
            wr(rows_a, every, out * gain)
    finish(len(sources) - 1)
    gate = rd(proj, every, 3)
    gate_buf[...] = (rd(rows_a, every) * (gate / (1.0 + jnp.exp(-gate)))).astype(BF16)
    if gather_out:
        m = n_mat - 1

        def take(s, carry):
            @pl.when(s < n_kv - 1)
            def _():
                forward_step(m, s)

            @pl.when(k - s >= 0)
            def _():
                @pl.when(s > 0)
                def _():
                    for d in range(1, n_grp):
                        y_wait(m, k - s, d)

                send_share(k - s)

            @pl.when(jnp.logical_and(s > 0, k + s < n_kv))
            def _():
                for d in range(1, n_grp):
                    y_wait(m, k + s, d)
                send_share(k + s)

            return carry

        lax.fori_loop(0, n_kv, take, 0)
    else:
        out_in.wait()
        for d in range(n_tp):
            send_share(lax.rem(t_me + d, n_tp))
    total = own_share[...]
    for d in range(1, n_tp):
        origin = lax.rem(t_me + d, n_tp)
        r_wait(origin)
        total = total + recv_buf[origin].astype(F32)
    mixed_ref[...] = total.reshape(seqs, props, feats).astype(BF16)

    for d in range(1, n_tp):
        t_copy(d).wait_send()
        r_copy(lax.rem(t_me + d, n_tp)).wait_send()

    def drain(m):
        def step(o, carry):
            @pl.when(jnp.logical_and(o <= k, k < n_kv - 1))
            def _():
                z_right(m, o).wait_send()

            @pl.when(jnp.logical_and(o >= k, k > 0))
            def _():
                z_left(m, o).wait_send()

            @pl.when(o != k)
            def _():
                for d in range(1, n_grp):
                    y_copy(m, o, d).wait_send()

            return carry

        lax.fori_loop(0, n_kv, step, 0)

    for m in range(n_mat):
        drain(m)


def body(
    sizes,
    tokens, in_gain, w_query, w_key, w_value, w_gate, w_beta, w_decay, decay_base, out_gain, w_out,
    state, prev_keys, prev_values, prev_beta, prev_decay, accepted,
):
    n_grp, n_kv, n_tp = sizes
    seqs, props, feats = tokens.shape
    heads = decay_base.shape[0]
    hd = out_gain.shape[0]
    width = heads * hd
    rows = seqs * props
    pad = 2 * props
    gather_out = n_kv == n_tp
    if not gather_out:
        w_out = lax.all_gather(w_out, "kv", axis=1, tiled=True)
        w_out = jnp.transpose(w_out.reshape(width, n_tp, feats), (1, 0, 2))
    n_mat = 5 if gather_out else 4
    cfg = (n_grp, n_kv, n_tp, seqs, props, heads, hd, gather_out)
    vmem = pl.BlockSpec(memory_space=pltpu.VMEM)
    hbm = pl.BlockSpec(memory_space=pltpu.HBM)
    args = (
        tokens, in_gain.reshape(1, -1), w_query, w_key, w_value, w_gate,
        w_beta.T, w_decay.T, decay_base.reshape(1, -1), out_gain.reshape(1, -1), w_out,
        state.reshape(seqs * hd, width), prev_keys, prev_values,
        jnp.transpose(prev_beta, (1, 2, 0)), jnp.transpose(prev_decay, (1, 2, 0)),
        accepted.reshape(1, seqs),
    )
    dma = pltpu.SemaphoreType.DMA
    mixed, new_state = pl.pallas_call(
        functools.partial(kernel, cfg),
        out_shape=(
            jax.ShapeDtypeStruct((seqs, props, feats), BF16),
            jax.ShapeDtypeStruct((seqs * hd, width), F32),
        ),
        in_specs=[hbm] * len(args),
        out_specs=(vmem, vmem),
        scratch_shapes=[
            *[pltpu.VMEM(args[i].shape, args[i].dtype) for i in (1, 6, 7, 8, 9, 12, 13, 14, 15, 16)],
            pltpu.VMEM((n_tp, seqs, props, feats), BF16),
            pltpu.VMEM((4, n_kv * w_key.shape[0], width), BF16),
            pltpu.VMEM((n_tp, width, feats), BF16),
            pltpu.VMEM((rows, n_tp * feats), BF16),
            pltpu.VMEM((width // 128, seqs * pad, 128), F32),
            pltpu.VMEM((width // 128, seqs * pad, 128), F32),
            pltpu.VMEM((width // 128, seqs * pad, 128), F32),
            pltpu.VMEM((width // 128, seqs * pad, 128), F32),
            pltpu.VMEM((seqs, width), F32),
            pltpu.VMEM((width // 128, rows, 128), F32),
            pltpu.VMEM((width // 128, rows, 128), F32),
            pltpu.VMEM((4, width // 128, rows, 128), F32),
            pltpu.VMEM((n_tp, rows, feats), BF16),
            pltpu.VMEM((n_tp, rows, feats), BF16),
            pltpu.VMEM((rows, width), BF16),
            pltpu.VMEM((rows, feats), F32),
            dma((2,)),
            dma((6,)),
            dma((n_mat, n_kv)),
            dma((n_mat, n_kv)),
            dma((n_mat, n_kv)),
            dma((max(n_grp - 1, 1), n_mat, n_kv)),
            dma((max(n_grp - 1, 1), n_mat, n_kv)),
            dma((n_tp - 1,)),
            dma((n_tp - 1,)),
            dma((n_tp,)),
            dma((n_tp,)),
            dma((10,)),
        ],
        compiler_params=pltpu.CompilerParams(
            collective_id=0, has_side_effects=True, vmem_limit_bytes=48 * 2**20),
    )(*args)
    return mixed, new_state.reshape(seqs, hd, width)


def solution(mesh):
    sizes = (mesh.shape["grp"], mesh.shape["kv"], mesh.shape["tp"])
    tokens = P(("grp", "kv"), None, "tp")
    placed = (
        tokens, P(), P("kv", "tp"), P("kv", "tp"), P("kv", "tp"), P("kv", "tp"), P(), P(),
        P("tp"), P(), P("tp", "kv"), tokens, tokens, tokens, tokens, tokens, P(("grp", "kv")),
    )
    return jax.shard_map(
        functools.partial(body, sizes),
        mesh=mesh,
        in_specs=placed,
        out_specs=(tokens, tokens),
        check_vma=False,
    )
```

```python
import functools

import jax
import jax.numpy as jnp
from jax import lax
from jax.experimental import pallas as pl
from jax.experimental.pallas import tpu as pltpu
from jax.sharding import PartitionSpec as P

EPS = 1e-06
F32 = jnp.float32
BF16 = jnp.bfloat16
MESH = pl.DeviceIdType.MESH


def kernel(
    cfg,
    tok_hbm, gain_hbm, wq_hbm, wk_hbm, wv_hbm, wg_hbm, wb_hbm, wd_hbm, base_hbm, og_hbm, wo_hbm,
    state_hbm, pk_hbm, pv_hbm, pb_hbm, pd_hbm, acc_hbm,
    mixed_ref, new_hbm,
    gain_ref, wb_ref, wd_ref, base_ref, og_ref, pk_ref, pv_ref, pb_ref, pd_ref, acc_ref, tok, wp, wo, st, normed, kq, res, tk, up, al, rows_a, rows_b, proj, send_buf, recv_buf, gate_buf, own_share,
    in_sem, own_sem, zr_send, zl_send, z_recv, y_send, y_recv, t_send, t_recv, r_send, r_recv,
    out_sem, small_sem,
):
    n_grp, n_kv, n_tp, seqs, props, heads, hd, gather_out = cfg
    width = heads * hd
    g = lax.axis_index("grp")
    k = lax.axis_index("kv")
    t_me = lax.axis_index("tp")
    rows = seqs * props
    own_rows = wk_hbm.shape[0]
    piece = own_rows // n_grp
    out_piece = wo.shape[1] // n_grp
    sources = [wk_hbm, wq_hbm, wv_hbm, wg_hbm]
    n_mat = len(sources) + (1 if gather_out else 0)

    tok_in = pltpu.make_async_copy(tok_hbm, tok.at[t_me], in_sem.at[0])
    tok_in.start()
    own_copies = []
    for m in range(n_mat):
        if m < len(sources):
            dst = wp.at[m, pl.ds(k * own_rows, own_rows), :]
            copy = pltpu.make_async_copy(sources[m], dst, own_sem.at[m])
        else:
            copy = pltpu.make_async_copy(wo_hbm, wo.at[k], own_sem.at[m])
        copy.start()
        own_copies.append(copy)
    early, late = [], []
    pairs = [
        (pk_hbm, pk_ref, early), (pv_hbm, pv_ref, early), (pb_hbm, pb_ref, early),
        (pd_hbm, pd_ref, early), (acc_hbm, acc_ref, early), (gain_hbm, gain_ref, late),
        (wb_hbm, wb_ref, late), (wd_hbm, wd_ref, late), (base_hbm, base_ref, late),
        (og_hbm, og_ref, late),
    ]
    for i, (src, dst, group) in enumerate(pairs):
        copy = pltpu.make_async_copy(src, dst, small_sem.at[i])
        copy.start()
        group.append(copy)
    state_in = pltpu.make_async_copy(state_hbm, st, in_sem.at[1])
    state_in.start()
    out_in = None
    if not gather_out:
        out_in = pltpu.make_async_copy(wo_hbm, wo, own_sem.at[n_mat])
        out_in.start()

    barrier = pltpu.get_barrier_semaphore()

    def greet(dev):
        pl.semaphore_signal(barrier, inc=1, device_id=dev, device_id_type=MESH)

    @pl.when(k > 0)
    def _():
        greet({"kv": k - 1})

    @pl.when(k < n_kv - 1)
    def _():
        greet({"kv": k + 1})

    for d in range(1, n_grp):
        greet({"grp": lax.rem(g + d, n_grp)})
    for d in range(1, n_tp):
        greet({"tp": lax.rem(t_me + d, n_tp)})

    beside = jnp.minimum(k, 1) + jnp.minimum(n_kv - 1 - k, 1)
    pl.semaphore_wait(barrier, n_grp + n_tp - 2 + beside)

    def slot(m, origin, part):
        if m < len(sources):
            return wp.at[m, pl.ds(origin * own_rows + part * piece, piece), :]
        return wo.at[origin, pl.ds(part * out_piece, out_piece), :]

    def z_right(m, origin):
        ref = slot(m, origin, g)
        return pltpu.make_async_remote_copy(
            ref, ref, zr_send.at[m, origin], z_recv.at[m, origin],
            device_id={"kv": k + 1}, device_id_type=MESH)

    def z_left(m, origin):
        ref = slot(m, origin, g)
        return pltpu.make_async_remote_copy(
            ref, ref, zl_send.at[m, origin], z_recv.at[m, origin],
            device_id={"kv": k - 1}, device_id_type=MESH)

    def y_copy(m, origin, d):
        ref = slot(m, origin, g)
        return pltpu.make_async_remote_copy(
            ref, ref, y_send.at[d - 1, m, origin], y_recv.at[d - 1, m, origin],
            device_id={"grp": lax.rem(g + d, n_grp)}, device_id_type=MESH)

    def y_wait(m, origin, d):
        ref = slot(m, origin, lax.rem(g + n_grp - d, n_grp))
        pltpu.make_async_remote_copy(
            ref, ref, y_send.at[d - 1, m, origin], y_recv.at[d - 1, m, origin],
            device_id={"grp": lax.rem(g + d, n_grp)}, device_id_type=MESH).wait_recv()

    def send_own(m):
        own_copies[m].wait()

        @pl.when(k < n_kv - 1)
        def _():
            z_right(m, k).start()

        @pl.when(k > 0)
        def _():
            z_left(m, k).start()

    def forward_step(m, s):
        left = k - 1 - s
        right = k + 1 + s

        @pl.when(left >= 0)
        def _():
            z_right(m, left).wait_recv()

            @pl.when(k < n_kv - 1)
            def _():
                z_right(m, left).start()

            for d in range(1, n_grp):
                y_copy(m, left, d).start()

        @pl.when(right < n_kv)
        def _():
            z_left(m, right).wait_recv()

            @pl.when(k > 0)
            def _():
                z_left(m, right).start()

            for d in range(1, n_grp):
                y_copy(m, right, d).start()

    def forward(m):
        def step(s, carry):
            forward_step(m, s)
            return carry

        lax.fori_loop(0, n_kv - 1, step, 0)

    def wait_y(m):
        def step(o, carry):
            @pl.when(o != k)
            def _():
                for d in range(1, n_grp):
                    y_wait(m, o, d)

            return carry

        lax.fori_loop(0, n_kv, step, 0)

    def t_copy(d):
        return pltpu.make_async_remote_copy(
            tok.at[t_me], tok.at[t_me], t_send.at[d - 1], t_recv.at[d - 1],
            device_id={"tp": lax.rem(t_me + d, n_tp)}, device_id_type=MESH)

    def t_wait(d):
        origin = lax.rem(t_me + n_tp - d, n_tp)
        pltpu.make_async_remote_copy(
            tok.at[origin], tok.at[origin], t_send.at[d - 1], t_recv.at[d - 1],
            device_id={"tp": lax.rem(t_me + d, n_tp)}, device_id_type=MESH).wait_recv()

    send_own(0)
    tok_in.wait()
    for d in range(1, n_tp):
        t_copy(d).start()
    send_own(1)
    send_own(2)

    blk = (
        lax.broadcasted_iota(jnp.int32, (width, width), 0) // hd
        == lax.broadcasted_iota(jnp.int32, (width, width), 1) // hd
    ).astype(F32).astype(BF16)
    lane_head = lax.broadcasted_iota(jnp.int32, (1, width), 1) // hd
    masks = [(lane_head == h).astype(F32) for h in range(heads)]

    def head_sum(x):
        hi = x.astype(BF16)
        lo = (x - hi.astype(F32)).astype(BF16)
        return jnp.dot(hi, blk, preferred_element_type=F32) + jnp.dot(
            lo, blk, preferred_element_type=F32)

    lanes = 128
    blocks = width // lanes

    def rd(ref, at, *lead):
        return jnp.concatenate([ref[(*lead, c, at)] for c in range(blocks)], axis=-1)

    def wr(ref, at, x, *lead):
        for c in range(blocks):
            ref[(*lead, c, at)] = x[:, c * lanes : (c + 1) * lanes]

    every = pl.ds(0, rows)

    pad = 2 * props

    def by_state(s, carry):
        tile = st[pl.ds(pl.multiple_of(s * hd, hd), hd), :]
        stacked = jnp.concatenate([(tile * mask).astype(BF16) for mask in masks], axis=0)
        at = pl.ds(pl.multiple_of(s * pad, pad), pad)
        lhs = rd(kq, at).astype(BF16)
        wr(res, at, jnp.dot(lhs, stacked, preferred_element_type=F32))
        return carry

    def solve(keys, values, weights, logs, queries):
        cumul = []
        run = None
        for t in range(props):
            run = logs[t] if run is None else run + logs[t]
            cumul.append(run)
        low = [(i, j) for i in range(props) for j in range(i)]
        products = [keys[i] * keys[j] for i, j in low]
        full = []
        if queries is not None:
            full = [(i, j) for i in range(props) for j in range(i + 1)]
            products += [queries[i] * keys[j] for i, j in full]
        sums = head_sum(jnp.concatenate(products, axis=0))
        sums = [sums[i * seqs : (i + 1) * seqs] for i in range(len(products))]
        kk = dict(zip(low, sums))
        qk = dict(zip(full, sums[len(low):]))
        dec = {pair: jnp.exp(cumul[pair[0]] - cumul[pair[1]]) for pair in low}
        growth = [jnp.exp(c) for c in cumul]
        update = []
        for t in range(props):
            seen = rd(res, pl.ds(t, seqs, stride=pad))
            term = values[t] - growth[t] * seen
            for j in range(t):
                term = term - kk[t, j] * dec[t, j] * update[j]
            update.append(weights[t] * term)
        outs = []
        if queries is not None:
            for t in range(props):
                out = growth[t] * rd(res, pl.ds(props + t, seqs, stride=pad))
                for j in range(t + 1):
                    score = qk[t, j] if j == t else qk[t, j] * dec[t, j]
                    out = out + score * update[j]
                outs.append(out)
        return cumul, growth, update, outs

    def split(ref):
        return [rd(ref, pl.ds(t, seqs, stride=props)) for t in range(props)]

    for copy in early:
        copy.wait()
    pk = pk_ref[...].astype(F32).reshape(rows, width)
    wr(rows_a, every, pk * lax.rsqrt(head_sum(pk * pk) + EPS))
    wr(rows_b, every, pv_ref[...].astype(F32).reshape(rows, width))
    keys = split(rows_a)
    values = split(rows_b)
    own_head = (
        lax.broadcasted_iota(jnp.int32, (heads, width), 0)
        == lax.broadcasted_iota(jnp.int32, (heads, width), 1) // hd
    ).astype(F32)

    def over_lanes(x):
        return lax.dot_general(
            x, own_head, (((0,), (0,)), ((), ())),
            precision=lax.Precision.HIGHEST, preferred_element_type=F32)

    weights, logs = [], []
    for t in range(props):
        live = (acc_ref[...] > t).astype(F32)
        weights.append(over_lanes(jax.nn.sigmoid(pb_ref[t]) * live))
        logs.append(over_lanes(pd_ref[t] * live))
        wr(kq, pl.ds(t, seqs, stride=pad), keys[t])
        wr(kq, pl.ds(props + t, seqs, stride=pad), keys[t])
    state_in.wait()
    lax.fori_loop(0, seqs, by_state, 0, unroll=4)
    cumul, growth, update, _ = solve(keys, values, weights, logs, None)
    al[...] = growth[-1]
    for t in range(props):
        wr(tk, pl.ds(t, seqs, stride=pad), jnp.exp(cumul[-1] - cumul[t]) * keys[t])
        wr(up, pl.ds(t, seqs, stride=pad), update[t])
        wr(tk, pl.ds(props + t, seqs, stride=pad), jnp.zeros((seqs, width), F32))
        wr(up, pl.ds(props + t, seqs, stride=pad), jnp.zeros((seqs, width), F32))

    def renew(s, carry):
        at = pl.ds(pl.multiple_of(s * pad, pad), pad)
        outer = lax.dot_general(
            rd(tk, at), rd(up, at), (((0,), (0,)), ((), ())), preferred_element_type=F32)
        where = pl.ds(pl.multiple_of(s * hd, hd), hd)
        tile = al[pl.ds(s, 1), :] * st[where, :]
        for h in range(heads):
            tile = tile + masks[h] * outer[h * hd : (h + 1) * hd, :]
        st[where, :] = tile
        return carry

    forward(0)
    send_own(3)
    lax.fori_loop(0, seqs // 2, renew, 0, unroll=2)
    forward(1)
    if gather_out:
        send_own(n_mat - 1)
    lax.fori_loop(seqs // 2, seqs, renew, 0, unroll=2)
    state_out = pltpu.make_async_copy(st, new_hbm, out_sem)
    state_out.start()

    for d in range(1, n_tp):
        t_wait(d)
    for copy in late:
        copy.wait()
    square = jnp.zeros((rows, 1), F32)
    for i in range(n_tp):
        wide = tok[i].astype(F32).reshape(rows, -1)
        square = square + jnp.sum(wide * wide, -1, keepdims=True)
    feats = tok.shape[3]
    scale = lax.rsqrt(square / (n_tp * feats) + EPS)
    for i in range(n_tp):
        cols = slice(i * feats, (i + 1) * feats)
        normed[:, cols] = (tok[i].astype(F32).reshape(rows, -1) * scale * gain_ref[:, cols]).astype(BF16)
    all_heads = wb_ref.shape[0]
    pick = (
        lax.broadcasted_iota(jnp.int32, (all_heads, width), 0)
        == t_me * heads + lax.broadcasted_iota(jnp.int32, (all_heads, width), 1) // hd
    ).astype(F32)

    def per_head(ref):
        raw = lax.dot_general(
            normed[...], ref[...], (((1,), (1,)), ((), ())), preferred_element_type=F32)
        return jnp.dot(raw, pick, precision=lax.Precision.HIGHEST, preferred_element_type=F32)

    wr(rows_a, every, jax.nn.sigmoid(per_head(wb_ref)))
    weights = split(rows_a)
    base = jnp.zeros((1, width), F32)
    for h in range(heads):
        base = jnp.where(lane_head == h, base_ref[:, h : h + 1], base)
    wr(rows_b, every, -base * jax.nn.softplus(per_head(wd_ref)))
    logs = split(rows_b)

    def project(m):
        return jnp.dot(normed[...], wp[m], preferred_element_type=F32)

    def finish(m):
        wait_y(m)
        if m < len(sources):
            value = project(m)
            if m == 0:
                value = value * lax.rsqrt(head_sum(value * value) + EPS)
            elif m == 1:
                value = value * lax.rsqrt(head_sum(value * value) + EPS) * hd ** (-0.5)
            wr(proj, every, value, m)

    outs = None
    def r_copy(dest):
        return pltpu.make_async_remote_copy(
            send_buf.at[dest], recv_buf.at[t_me], r_send.at[dest], r_recv.at[t_me],
            device_id={"tp": dest}, device_id_type=MESH)

    def r_wait(origin):
        pltpu.make_async_remote_copy(
            send_buf.at[origin], recv_buf.at[origin], r_send.at[origin], r_recv.at[origin],
            device_id={"tp": origin}, device_id_type=MESH).wait_recv()

    def send_share(dest):
        share = jnp.dot(gate_buf[...], wo[dest], preferred_element_type=F32)

        @pl.when(dest == t_me)
        def _():
            own_share[...] = share

        @pl.when(dest != t_me)
        def _():
            send_buf[dest] = share.astype(BF16)
            r_copy(dest).start()

    for m in range(len(sources)):
        if m >= 2:
            forward(m)
        if m >= 1:
            finish(m - 1)
        if m == 3:
            keys = [rd(proj, pl.ds(t, seqs, stride=props), 0) for t in range(props)]
            queries = [rd(proj, pl.ds(t, seqs, stride=props), 1) for t in range(props)]
            values = [rd(proj, pl.ds(t, seqs, stride=props), 2) for t in range(props)]
            for t in range(props):
                wr(kq, pl.ds(t, seqs, stride=pad), keys[t])
                wr(kq, pl.ds(props + t, seqs, stride=pad), queries[t])
            lax.fori_loop(0, seqs, by_state, 0, unroll=4)
            outs = solve(keys, values, weights, logs, queries)[3]
            for t in range(props):
                wr(rows_a, pl.ds(t, seqs, stride=props), outs[t])
            out = rd(rows_a, every)
            out = out * lax.rsqrt(head_sum(out * out) / hd + EPS)
            tile_gain = (
                lax.broadcasted_iota(jnp.int32, (hd, width), 0)
                == lax.broadcasted_iota(jnp.int32, (hd, width), 1) % hd
            ).astype(F32)
            gain = jnp.dot(
                jnp.broadcast_to(og_ref[...], (8, hd)), tile_gain,
                precision=lax.Precision.HIGHEST, preferred_element_type=F32)[:1]
            wr(rows_a, every, out * gain)
    finish(len(sources) - 1)
    gate = rd(proj, every, 3)
    gate_buf[...] = (rd(rows_a, every) * (gate / (1.0 + jnp.exp(-gate)))).astype(BF16)
    if gather_out:
        m = n_mat - 1

        def take(s, carry):
            @pl.when(s < n_kv - 1)
            def _():
                forward_step(m, s)

            @pl.when(k - s >= 0)
            def _():
                @pl.when(s > 0)
                def _():
                    for d in range(1, n_grp):
                        y_wait(m, k - s, d)

                send_share(k - s)

            @pl.when(jnp.logical_and(s > 0, k + s < n_kv))
            def _():
                for d in range(1, n_grp):
                    y_wait(m, k + s, d)
                send_share(k + s)

            return carry

        lax.fori_loop(0, n_kv, take, 0)
    else:
        out_in.wait()
        for d in range(n_tp):
            send_share(lax.rem(t_me + d, n_tp))
    total = own_share[...]
    for d in range(1, n_tp):
        origin = lax.rem(t_me + d, n_tp)
        r_wait(origin)
        total = total + recv_buf[origin].astype(F32)
    mixed_ref[...] = total.reshape(seqs, props, feats).astype(BF16)

    for d in range(1, n_tp):
        t_copy(d).wait_send()
        r_copy(lax.rem(t_me + d, n_tp)).wait_send()

    def drain(m):
        def step(o, carry):
            @pl.when(jnp.logical_and(o <= k, k < n_kv - 1))
            def _():
                z_right(m, o).wait_send()

            @pl.when(jnp.logical_and(o >= k, k > 0))
            def _():
                z_left(m, o).wait_send()

            @pl.when(o != k)
            def _():
                for d in range(1, n_grp):
                    y_copy(m, o, d).wait_send()

            return carry

        lax.fori_loop(0, n_kv, step, 0)

    for m in range(n_mat):
        drain(m)
    state_out.wait()


def body(
    sizes,
    tokens, in_gain, w_query, w_key, w_value, w_gate, w_beta, w_decay, decay_base, out_gain, w_out,
    state, prev_keys, prev_values, prev_beta, prev_decay, accepted,
):
    n_grp, n_kv, n_tp = sizes
    seqs, props, feats = tokens.shape
    heads = decay_base.shape[0]
    hd = out_gain.shape[0]
    width = heads * hd
    rows = seqs * props
    pad = 2 * props
    gather_out = n_kv == n_tp
    if not gather_out:
        w_out = lax.all_gather(w_out, "kv", axis=1, tiled=True)
        w_out = jnp.transpose(w_out.reshape(width, n_tp, feats), (1, 0, 2))
    n_mat = 5 if gather_out else 4
    cfg = (n_grp, n_kv, n_tp, seqs, props, heads, hd, gather_out)
    vmem = pl.BlockSpec(memory_space=pltpu.VMEM)
    hbm = pl.BlockSpec(memory_space=pltpu.HBM)
    args = (
        tokens, in_gain.reshape(1, -1), w_query, w_key, w_value, w_gate,
        w_beta.T, w_decay.T, decay_base.reshape(1, -1), out_gain.reshape(1, -1), w_out,
        state.reshape(seqs * hd, width), prev_keys, prev_values,
        jnp.transpose(prev_beta, (1, 2, 0)), jnp.transpose(prev_decay, (1, 2, 0)),
        accepted.reshape(1, seqs),
    )
    dma = pltpu.SemaphoreType.DMA
    mixed, new_state = pl.pallas_call(
        functools.partial(kernel, cfg),
        out_shape=(
            jax.ShapeDtypeStruct((seqs, props, feats), BF16),
            jax.ShapeDtypeStruct((seqs * hd, width), F32),
        ),
        in_specs=[hbm] * len(args),
        out_specs=(vmem, pl.BlockSpec(memory_space=pl.ANY)),
        scratch_shapes=[
            *[pltpu.VMEM(args[i].shape, args[i].dtype) for i in (1, 6, 7, 8, 9, 12, 13, 14, 15, 16)],
            pltpu.VMEM((n_tp, seqs, props, feats), BF16),
            pltpu.VMEM((4, n_kv * w_key.shape[0], width), BF16),
            pltpu.VMEM((n_tp, width, feats), BF16),
            pltpu.VMEM((seqs * hd, width), F32),
            pltpu.VMEM((rows, n_tp * feats), BF16),
            pltpu.VMEM((width // 128, seqs * pad, 128), F32),
            pltpu.VMEM((width // 128, seqs * pad, 128), F32),
            pltpu.VMEM((width // 128, seqs * pad, 128), F32),
            pltpu.VMEM((width // 128, seqs * pad, 128), F32),
            pltpu.VMEM((seqs, width), F32),
            pltpu.VMEM((width // 128, rows, 128), F32),
            pltpu.VMEM((width // 128, rows, 128), F32),
            pltpu.VMEM((4, width // 128, rows, 128), F32),
            pltpu.VMEM((n_tp, rows, feats), BF16),
            pltpu.VMEM((n_tp, rows, feats), BF16),
            pltpu.VMEM((rows, width), BF16),
            pltpu.VMEM((rows, feats), F32),
            dma((2,)),
            dma((6,)),
            dma((n_mat, n_kv)),
            dma((n_mat, n_kv)),
            dma((n_mat, n_kv)),
            dma((max(n_grp - 1, 1), n_mat, n_kv)),
            dma((max(n_grp - 1, 1), n_mat, n_kv)),
            dma((n_tp - 1,)),
            dma((n_tp - 1,)),
            dma((n_tp,)),
            dma((n_tp,)),
            dma(()),
            dma((10,)),
        ],
        compiler_params=pltpu.CompilerParams(
            collective_id=0, has_side_effects=True, vmem_limit_bytes=67043328),
    )(*args)
    return mixed, new_state.reshape(seqs, hd, width)


def solution(mesh):
    sizes = (mesh.shape["grp"], mesh.shape["kv"], mesh.shape["tp"])
    tokens = P(("grp", "kv"), None, "tp")
    placed = (
        tokens, P(), P("kv", "tp"), P("kv", "tp"), P("kv", "tp"), P("kv", "tp"), P(), P(),
        P("tp"), P(), P("tp", "kv"), tokens, tokens, tokens, tokens, tokens, P(("grp", "kv")),
    )
    return jax.shard_map(
        functools.partial(body, sizes),
        mesh=mesh,
        in_specs=placed,
        out_specs=(tokens, tokens),
        check_vma=False,
    )
```
